512 devices in a mesh: sp: 64 (over z, y), tp: 8 (over x, core).
Axes of the slice: x: 4, y: 4, z: 16, core: 2. Of those that a mesh axis runs over, the one named last changes fastest.
Arguments:
- tokens: bfloat16 [32768, 3072], P('sp'), may hold values from -72 to 72
- w_query: bfloat16 [3072, 1024], P('sp', 'tp'), may hold values from -0.109375 to 0.109375
- w_key: bfloat16 [3072, 1024], P('sp', 'tp'), may hold values from -0.109375 to 0.109375
- w_value: bfloat16 [3072, 1024], P('sp', 'tp'), may hold values from -0.4375 to 0.4375
- w_out: bfloat16 [1024, 3072], P('tp', 'sp'), may hold values from -0.1875 to 0.1875
Outputs:
- mixed: bfloat16 [32768, 3072], P(('sp', 'tp'))
- row_lse: float32 [16, 32768], P('tp', 'sp')
The draws below stay inside these ranges and needn't reach their ends.
All inputs are finite; a program needn't handle non-finite values.
Results may differ from the reference program's by a relative error of at most 0.014.
Values may be sent and summed in bfloat16 or wider, within the bound.
A program may use at most 64 MiB of HBM per device.

```python
import jax
import jax.numpy as jnp
from jax import lax

D = 3072
HEADS = 16
HEAD_SIZE = 64
KEYS_BEHIND = 128
D_ATT = 1024
SEQUENCE_TOKENS = 32768
N_TP = 8


def draw_tokens(key, part):
    base_offset = jax.random.truncated_normal(key, -6.0, 6.0, (SEQUENCE_TOKENS, D), jnp.float32)
    return base_offset.astype(jnp.bfloat16)


def block_levels(own_key, extent, pieces, least, high):
    factor_of = 1.0
    for dim, blocks in pieces:
        steps = jax.random.uniform(jax.random.fold_in(jax.random.fold_in(own_key, 6), dim), (blocks,), jnp.float32, least / len(pieces), high / len(pieces))
        factor_of = factor_of * jnp.repeat(jnp.exp(steps), extent[dim] // blocks).reshape((-1,) + (1,) * (len(extent) - 1 - dim))
    return factor_of


def centred(key, extent, spread, bound, pieces=(), held_as=jnp.bfloat16):
    result = jax.random.normal(key, extent, jnp.float32) * spread
    if len(pieces) > 0:
        result = block_levels(key, extent, pieces, -0.22, 0.18) * result
    return jnp.clip(result, min=-bound, max=bound).astype(held_as)


def setup_inputs(seed: int = 0) -> dict:
    arg_keys = jax.random.split(jax.random.key(seed), 6)
    tokens = draw_tokens(jax.random.fold_in(arg_keys[5], 71), 0)
    w_query = centred(arg_keys[1], (D, D_ATT), D ** -0.5, 0.109375, ((0, 64), (1, 8)))
    w_key = centred(arg_keys[2], (D, D_ATT), D ** -0.5, 0.109375, ((0, 64), (1, 8)))
    w_value = centred(arg_keys[3], (D, D_ATT), (D // 16) ** -0.5, 0.4375, ((0, 64), (1, 8)))
    w_out = centred(arg_keys[4], (D_ATT, D), D_ATT ** -0.5, 0.1875, ((0, 8), (1, 64)))
    return {"tokens": tokens, "w_query": w_query, "w_key": w_key, "w_value": w_value, "w_out": w_out}


dilation_rates = (1, 4, 16)
neg_big = -1e30


def band(query_class_rows, key_class_rows, value_class_rows, key_first_index):
    sequence_length = query_class_rows.shape[0]
    if sequence_length <= KEYS_BEHIND:
        blocks = 1
        step = sequence_length
        q_blk = query_class_rows[None]
        k_blk = key_class_rows[None]
        v_blk = value_class_rows[None]
    else:
        blocks = sequence_length // KEYS_BEHIND
        step = KEYS_BEHIND
        q_blk = query_class_rows.reshape(blocks, KEYS_BEHIND, HEAD_SIZE)
        k_rows = key_class_rows.reshape(blocks + 1, KEYS_BEHIND, HEAD_SIZE)
        v_rows = value_class_rows.reshape(blocks + 1, KEYS_BEHIND, HEAD_SIZE)
        k_blk = jnp.concatenate([k_rows[:-1], k_rows[1:]], axis=1)
        v_blk = jnp.concatenate([v_rows[:-1], v_rows[1:]], axis=1)
    score = jnp.einsum('nqd,nkd->nqk', q_blk.astype(jnp.float32), k_blk.astype(jnp.float32)) * (HEAD_SIZE ** -0.5)
    row_at = jnp.arange(step, dtype=jnp.int32)[:, None]
    col_at = jnp.arange(k_blk.shape[1], dtype=jnp.int32)[None, :]
    dist = KEYS_BEHIND + row_at - col_at
    key_pos = key_first_index + jnp.arange(blocks, dtype=jnp.int32)[:, None, None] * step + col_at[None]
    mask = (dist >= 0) & (dist <= KEYS_BEHIND) & (key_pos >= 0)
    score = jnp.where(mask, score, neg_big)
    top = jnp.max(score, axis=-1, keepdims=True)
    weight = jnp.exp(score - top)
    denom = jnp.sum(weight, axis=-1)
    weight_bf = weight.astype(jnp.bfloat16)
    out = jnp.einsum('nqk,nkd->nqd', weight_bf.astype(jnp.float32), v_blk.astype(jnp.float32)) / denom[..., None]
    lse = top[..., 0] + jnp.log(denom)
    return out.reshape(sequence_length, HEAD_SIZE), lse.reshape(sequence_length)


def one_head(parts):
    query_head_rows, key_head_rows, value_head_rows = parts
    outs = []
    lses = []
    for dilation_rate in dilation_rates:
        sequence_length = SEQUENCE_TOKENS // dilation_rate
        query_class_rows = query_head_rows.reshape(sequence_length, dilation_rate, HEAD_SIZE).transpose(1, 0, 2)
        padding_rows = jnp.zeros((KEYS_BEHIND * dilation_rate, HEAD_SIZE), jnp.bfloat16)
        key_class_rows = jnp.concatenate([padding_rows, key_head_rows], 0).reshape(KEYS_BEHIND + sequence_length, dilation_rate, HEAD_SIZE).transpose(1, 0, 2)
        value_class_rows = jnp.concatenate([padding_rows, value_head_rows], 0).reshape(KEYS_BEHIND + sequence_length, dilation_rate, HEAD_SIZE).transpose(1, 0, 2)
        out, lse = jax.vmap(lambda a, b, c: band(a, b, c, -KEYS_BEHIND))(query_class_rows, key_class_rows, value_class_rows)
        outs.append(out.transpose(1, 0, 2).reshape(SEQUENCE_TOKENS, HEAD_SIZE))
        lses.append(lse.T.reshape(SEQUENCE_TOKENS))
    lse_all = jnp.stack(lses, 0)
    peak = jnp.max(lse_all, axis=0)
    expo = jnp.exp(lse_all - peak)
    total = jnp.sum(expo, axis=0)
    mix = expo / total
    attended = jnp.sum(mix[..., None] * jnp.stack(outs, 0), axis=0)
    return attended, peak + jnp.log(total)


def reference(tokens, w_query, w_key, w_value, w_out):
    query_input = jnp.dot(tokens, w_query, preferred_element_type=jnp.float32).astype(jnp.bfloat16)
    keys = jnp.dot(tokens, w_key, preferred_element_type=jnp.float32).astype(jnp.bfloat16)
    values = jnp.dot(tokens, w_value, preferred_element_type=jnp.float32).astype(jnp.bfloat16)

    def heads_first(a):
        return a.reshape(SEQUENCE_TOKENS, HEADS, HEAD_SIZE).transpose(1, 0, 2)

    attended, row_lse = lax.map(one_head, (heads_first(query_input), heads_first(keys), heads_first(values)))
    attended = attended.transpose(1, 0, 2).reshape(SEQUENCE_TOKENS, D_ATT).astype(jnp.bfloat16)
    cols = D_ATT // N_TP
    total = jnp.zeros((SEQUENCE_TOKENS, D), jnp.float32)
    for group in range(N_TP):
        part = jnp.dot(attended[:, group * cols:(group + 1) * cols], w_out[group * cols:(group + 1) * cols],
                       preferred_element_type=jnp.float32).astype(jnp.bfloat16)
        total = total + part.astype(jnp.float32)
    return total.astype(jnp.bfloat16), row_lse
```

```python
import jax
import jax.numpy as jnp
from jax import lax
from jax.experimental import pallas as pl
from jax.experimental.pallas import tpu as pltpu
from jax.sharding import Mesh
from jax.sharding import PartitionSpec as P

HEAD = 64
WINDOW = 128
NZ = 16
NY = 4
NX = 4
MESH = pl.DeviceIdType.MESH
SP = ("z", "y")
TP = ("x", "c")
NEG = -1e30
LN2 = 0.6931471805599453
F32 = jnp.float32
BF16 = jnp.bfloat16


def nt_dot(a, b):
    return lax.dot_general(a, b, (((1,), (1,)), ((), ())), preferred_element_type=F32)


def remote(src, dst, send, recv, device):
    return pltpu.make_async_remote_copy(
        src_ref=src, dst_ref=dst, send_sem=send, recv_sem=recv, device_id=device, device_id_type=MESH
    )


def layer_kernel(
    tokens, wq, wk, wv, wo, mixed, lse_out,
    tok, wkv, wqo, wox, halo, qf, kvf, oa, ma, la, att, lse_rows, att_b, att_x, part, part_b, part_x,
    bias_a, bias_b,
    tok_sem, kvy_s, kvy_r, zs, zr, ys, yr, xs, xr, hs, hr, as_, ar, cs, cr,
):
    z, y, x, c = (lax.axis_index(n) for n in ("z", "y", "x", "c"))
    sp = z * NY + y
    shard, lanes = wk.shape
    rows = tokens.shape[0]
    copy_tokens = pltpu.make_async_copy(tokens, tok, tok_sem)
    copy_tokens.start()

    def at_z(d):
        return lax.rem(z + d + NZ, NZ)

    def at_y(d):
        return lax.rem(y + d + NY, NY)

    def at_x(d):
        return lax.rem(x + d + NX, NX)

    wkv[sp, :, 0:lanes] = wk[...]
    wkv[sp, :, lanes:] = wv[...]
    wqo[sp, :, 0:lanes] = wq[...]
    wqo[sp, :, lanes:] = wo[...]

    barrier = pltpu.get_barrier_semaphore()
    peers = [{"z": at_z(1)}, {"z": at_z(-1)}]
    peers += [{"y": at_y(d)} for d in range(1, NY)]
    peers += [{"x": at_x(d)} for d in range(1, NX)]
    peers += [{"c": 1 - c}]
    for peer in peers:
        pl.semaphore_signal(barrier, inc=1, device_id=peer, device_id_type=MESH)
    pl.semaphore_wait(barrier, len(peers))

    sends = []

    def start(cp):
        cp.start()
        sends.append(cp)

    z_up, z_dn = {"z": at_z(1)}, {"z": at_z(-1)}
    y_up, y_dn = {"y": at_y(1)}, {"y": at_y(-1)}

    def half(ref, flow, h):
        part_ = pl.ds(h * lanes, lanes)
        return ref.at[:, :, part_] if flow == 0 else ref.at[:, part_]

    def z_block(flow, src):
        return wkv.at[pl.ds(src * NY, NY)] if flow == 0 else wqo.at[src * NY + y]

    last = NZ // 2

    def z_copy(flow, way, s, src_z):
        ref = z_block(flow, src_z)
        if s == last:
            ref = half(ref, flow, way)
        return remote(ref, ref, zs.at[flow, way, s - 1], zr.at[flow, way, s - 1], z_up if way == 0 else z_dn)

    def z_send(flow, way, s):
        start(z_copy(flow, way, s, at_z(-(s - 1) if way == 0 else s - 1)))

    def z_wait(flow, way, s):
        z_copy(flow, way, s, at_z(-s if way == 0 else s)).wait_recv()

    def y_copy(kind, slot, col):
        src_z = at_z(-slot)
        ref = wqo.at[src_z * NY + at_y(col)]
        if kind >= 2:
            ref = half(ref, 1, kind - 2)
        return remote(ref, ref, ys.at[kind, slot], yr.at[kind, slot], y_up if kind % 2 == 0 else y_dn)

    def y_send(slot):
        start(y_copy(0, slot, 0))
        start(y_copy(1, slot, 0))

    def y_relay(slot):
        y_copy(0, slot, -1).wait_recv()
        start(y_copy(2, slot, -1))
        y_copy(1, slot, 1).wait_recv()
        start(y_copy(3, slot, 1))

    def y_done(slot):
        y_copy(2, slot, 2).wait_recv()
        y_copy(3, slot, 2).wait_recv()

    def kv_row(d, col):
        ref = wkv.at[sp + 0 * col] if col is None else wkv.at[z * NY + at_y(col)]
        return remote(ref, ref, kvy_s.at[d - 1], kvy_r.at[d - 1], {"y": at_y(d)})

    for d in (1, 3, 2):
        start(kv_row(d, 0))
    z_send(1, 0, 1)
    z_send(1, 1, 1)
    y_send(0)
    for d in (1, 3, 2):
        kv_row(d, -d).wait_recv()
    z_send(0, 0, 1)
    z_send(0, 1, 1)
    waiting = [0]
    for s in range(1, last + 1):
        for way in (0, 1):
            z_wait(1, way, s)
            if s < last:
                z_send(1, way, s + 1)
        arrived = [s, NZ - s] if s < last else [s]
        for slot in arrived:
            y_send(slot)
        for way in (0, 1):
            z_wait(0, way, s)
            if s < last:
                z_send(0, way, s + 1)
        for slot in waiting:
            y_relay(slot)
        waiting = arrived
    for slot in waiting:
        y_relay(slot)
    for slot in range(NZ):
        y_done(slot)

    chunks = wox.shape[1] // 16
    def x_copy(kind, k, rel):
        span = pl.ds(k * 16, 16)
        src = wqo.at[span, :, pl.ds(lanes, lanes)] if rel is None else wox.at[rel, span]
        place = {0: NX - 2, 1: 0, 2: 1, 3: 1}[kind]
        dst = wox.at[place, span]
        to = {"x": at_x(1)} if kind % 2 == 0 else {"x": at_x(-1)}
        j = kind if kind < 2 else 2
        return remote(src, dst, xs.at[j, k], xr.at[j, k], to)

    for k in range(chunks):
        start(x_copy(0, k, None))
        start(x_copy(1, k, None))

    def x_relay(k):
        up = k < chunks // 2
        x_copy(0, k, None).wait_recv()
        if up:
            start(x_copy(2, k, 2))
        x_copy(1, k, None).wait_recv()
        if not up:
            start(x_copy(3, k, 0))

    copy_tokens.wait()
    kv = jnp.dot(tok[...], wkv[...].reshape(NZ * NY * shard, 2 * lanes), preferred_element_type=F32)
    for j in range(2):
        side = slice(j * lanes, (j + 1) * lanes)
        kvf[j, WINDOW:, :] = kv[:, side]
        for e in range(4):
            for b in range(4):
                picked = kvf[j, pl.ds(WINDOW + 4 * b + e, 32, stride=16), :]
                halo[e, 0, 32 * b:32 * b + 32, side] = picked.astype(BF16)

    def prev_copy(e):
        return remote(halo.at[e, 0], halo.at[e, 4], hs.at[0, e], hr.at[0, e], z_up)

    def row_copy(e, k, src):
        return remote(halo.at[e, src], halo.at[e, k], hs.at[k, e], hr.at[k, e], {"y": at_y(k)})

    for e in range(4):
        prev_copy(e).start()
    for k in (1, 3, 2):
        @pl.when(y + k < NY)
        def _():
            for e in range(4):
                row_copy(e, k, 0).start()

    q = jnp.dot(tok[...], wqo[:, :, 0:lanes].reshape(NZ * NY * shard, lanes), preferred_element_type=F32)
    qf[...] = q.astype(BF16).astype(F32) * (HEAD ** -0.5)

    r = lax.broadcasted_iota(jnp.int32, (WINDOW, 2 * WINDOW), 0)
    k_ = lax.broadcasted_iota(jnp.int32, (WINDOW, 2 * WINDOW), 1)
    dist = WINDOW + r - k_
    near = (dist >= 0) & (dist <= WINDOW)
    bias_a[1] = jnp.where(near, 0.0, NEG)
    bias_a[0] = jnp.where(near & ((k_ >= WINDOW) | (sp > 0)), 0.0, NEG)
    r = lax.broadcasted_iota(jnp.int32, (WINDOW, 5 * WINDOW), 0)
    k_ = lax.broadcasted_iota(jnp.int32, (WINDOW, 5 * WINDOW), 1)
    back = lax.shift_right_logical(k_, 7)
    kr = k_ & 127
    db = lax.shift_right_logical(r, 5) - lax.shift_right_logical(kr, 5)
    dist = rows * back + 16 * ((r & 31) - (kr & 31)) + 4 * db
    seen = (dist >= 0) & (back <= sp)
    in16 = seen & (db == 0) & (dist <= 16 * WINDOW)
    in4 = seen & (dist <= 4 * WINDOW)
    bias_b[...] = jnp.where(in16 & in4, LN2, jnp.where(in16 | in4, 0.0, NEG))

    for e in range(4):
        prev_copy(e).wait_recv()
        for k in (1, 3, 2):
            @pl.when(y + k >= NY)
            def _():
                row_copy(e, k, 4).start()

    head0 = lax.broadcasted_iota(jnp.int32, (WINDOW, lanes), 1) < HEAD

    def attend(qb, kb, vb, bias):
        q0 = jnp.where(head0, qb, 0.0).astype(BF16)
        q1 = jnp.where(head0, 0.0, qb).astype(BF16)
        s = nt_dot(jnp.concatenate([q0, q1], 0), kb)
        probs, tops, sums = [], [], []
        for h in range(2):
            sh = s[h * WINDOW:(h + 1) * WINDOW] + bias
            top = jnp.max(sh, axis=1, keepdims=True)
            w = jnp.exp(sh - top)
            tops.append(top)
            sums.append(jnp.sum(w, axis=1, keepdims=True))
            probs.append(w.astype(BF16))
        o = jnp.dot(jnp.concatenate(probs, 0), vb, preferred_element_type=F32)
        out = jnp.where(head0, o[0:WINDOW], o[WINDOW:])
        return out, jnp.where(head0, tops[0], tops[1]), jnp.where(head0, sums[0], sums[1])

    for e in range(4):
        row_copy(e, 1, 0).wait_recv()
    for e in range(4):
        for b in range(4):
            for j in range(2):
                tail = halo[e, 1, 32 * b + 24:32 * b + 32, j * lanes:(j + 1) * lanes]
                kvf[j, pl.ds(4 * b + e, 8, stride=16), :] = tail.astype(F32)
    for i in range(rows // WINDOW):
        span = slice(i * WINDOW, (i + 1) * WINDOW)
        keys = slice(i * WINDOW, (i + 2) * WINDOW)
        out, top, total = attend(
            qf[span, :], kvf[0, keys, :].astype(BF16), kvf[1, keys, :].astype(BF16), bias_a[min(i, 1)]
        )
        oa[span, :] = out
        ma[span, :] = top
        la[span, :] = total

    for k in range(chunks):
        x_relay(k)

    for e in range(4):
        row_copy(e, 3, 0).wait_recv()
        row_copy(e, 2, 0).wait_recv()
        pick = [pl.ds(4 * b + e, 32, stride=16) for b in range(4)]
        qb = jnp.concatenate([qf[p, :] for p in pick], 0)
        kvb = halo[e].reshape(5 * WINDOW, 2 * lanes)
        out, top, total = attend(qb, kvb[:, 0:lanes], kvb[:, lanes:], bias_b[...])
        o_a = jnp.concatenate([oa[p, :] for p in pick], 0)
        m_a = jnp.concatenate([ma[p, :] for p in pick], 0)
        l_a = jnp.concatenate([la[p, :] for p in pick], 0)
        peak = jnp.maximum(top, m_a)
        f_b = jnp.exp(top - peak)
        f_a = jnp.exp(m_a - peak)
        denom = f_a * l_a + f_b * total
        res = (f_a * o_a + f_b * out) / denom
        lse = peak + jnp.log(denom)
        for b in range(4):
            att[pick[b], :] = res[32 * b:32 * b + 32]
            lse_rows[pick[b], :] = lse[32 * b:32 * b + 32]

    att_b[...] = att[...].reshape(NX, rows // NX, lanes).astype(BF16)

    def att_copy(d):
        return remote(att_b.at[at_x(d)], att_x.at[NX - d], as_.at[d - 1], ar.at[d - 1], {"x": at_x(d)})

    for d in (1, 3, 2):
        start(att_copy(d))
    att_x[0] = att_b[x]
    lse_t = lse_rows[...].T
    lse_out[0:1, :] = lse_t[0:1, :]
    lse_out[1:2, :] = lse_t[HEAD:HEAD + 1, :]
    for k in range(chunks):
        x_copy(2 if k < chunks // 2 else 3, k, 0).wait_recv()
    for d in (1, 3, 2):
        att_copy(d).wait_recv()

    groups = 8
    width = NZ * NY // groups
    hrows = rows // NX // 2

    def core_copy(j):
        return remote(part_b.at[j, 1 - c], part_x.at[j], cs.at[j], cr.at[j], {"c": 1 - c})

    for g in range(groups):
        span = slice(g * width, (g + 1) * width)
        w0 = wqo[span, :, lanes:].reshape(width * shard, lanes)
        acc = nt_dot(att_x[0], w0)
        for k in range(1, NX):
            acc += nt_dot(att_x[k], wox[k - 1, span].reshape(width * shard, lanes))
        acc = acc.reshape(2, hrows, width * shard)
        part[g] = acc
        part_b[g] = acc.astype(BF16)
        start(core_copy(g))
    for g in range(groups):
        core_copy(g).wait_recv()
        mixed[:, g * width * shard:(g + 1) * width * shard] = (part[g, c] + part_x[g].astype(F32)).astype(BF16)

    for e in range(4):
        prev_copy(e).wait_send()
        for k in (1, 2, 3):
            row_copy(e, k, 0).wait_send()
    for cp in sends:
        cp.wait_send()


def shards(tokens, w_query, w_key, w_value, w_out):
    rows, depth = tokens.shape
    shard, lanes = w_query.shape
    n_sp = NZ * NY
    groups = 8
    wide = n_sp // groups * shard
    vmem = pl.BlockSpec(memory_space=pltpu.VMEM)
    dma = pltpu.SemaphoreType.DMA
    return pl.pallas_call(
        layer_kernel,
        name="layer",
        out_shape=(
            jax.ShapeDtypeStruct((rows // 8, depth), BF16),
            jax.ShapeDtypeStruct((2, rows), F32),
        ),
        in_specs=[pl.BlockSpec(memory_space=pl.ANY)] + [vmem] * 4,
        out_specs=(vmem, vmem),
        scratch_shapes=[
            pltpu.VMEM((rows, depth), BF16),
            pltpu.VMEM((n_sp, shard, 2 * lanes), BF16),
            pltpu.VMEM((n_sp, shard, 2 * lanes), BF16),
            pltpu.VMEM((NX - 1, n_sp, shard, lanes), BF16),
            pltpu.VMEM((4, 5, WINDOW, 2 * lanes), BF16),
            pltpu.VMEM((rows, lanes), F32),
            pltpu.VMEM((2, WINDOW + rows, lanes), F32),
            pltpu.VMEM((rows, lanes), F32),
            pltpu.VMEM((rows, lanes), F32),
            pltpu.VMEM((rows, lanes), F32),
            pltpu.VMEM((rows, lanes), F32),
            pltpu.VMEM((rows, lanes), F32),
            pltpu.VMEM((NX, rows // NX, lanes), BF16),
            pltpu.VMEM((NX, rows // NX, lanes), BF16),
            pltpu.VMEM((groups, 2, rows // NX // 2, wide), F32),
            pltpu.VMEM((groups, 2, rows // NX // 2, wide), BF16),
            pltpu.VMEM((groups, rows // NX // 2, wide), BF16),
            pltpu.VMEM((2, WINDOW, 2 * WINDOW), F32),
            pltpu.VMEM((WINDOW, 5 * WINDOW), F32),
            dma,
            dma((3,)), dma((3,)),
            dma((2, 2, NZ // 2)), dma((2, 2, NZ // 2)),
            dma((4, NZ)), dma((4, NZ)),
            dma((3, 4)), dma((3, 4)),
            dma((4, 4)), dma((4, 4)),
            dma((3,)), dma((3,)),
            dma((groups,)), dma((groups,)),
        ],
        compiler_params=pltpu.CompilerParams(
            collective_id=0, has_side_effects=True, vmem_limit_bytes=60 * 1024 * 1024
        ),
    )(tokens, w_query, w_key, w_value, w_out.T)


def solution(mesh):
    torus = Mesh(mesh.devices.reshape(NZ, NY, NX, 2), ("z", "y", "x", "c"))
    in_specs = (P(SP, None), P(SP, TP), P(SP, TP), P(SP, TP), P(TP, SP))
    out_specs = (P(SP + TP, None), P(TP, SP))
    return jax.shard_map(
        shards, mesh=torus, in_specs=in_specs, out_specs=out_specs, check_vma=False
    )
```

```python
import jax
import jax.numpy as jnp
from jax import lax
from jax.experimental import pallas as pl
from jax.experimental.pallas import tpu as pltpu
from jax.sharding import Mesh
from jax.sharding import PartitionSpec as P

HEAD = 64
WINDOW = 128
NZ = 16
NY = 4
NX = 4
MESH = pl.DeviceIdType.MESH
SP = ("z", "y")
TP = ("x", "c")
NEG = -1e30
LN2 = 0.6931471805599453
F32 = jnp.float32
BF16 = jnp.bfloat16
Z_PARTS = [(0, 2), (2, 1)]
LAST_PARTS = [[(0, 2)], [(2, 1)]]
O_PARTS = [(0, 2), (2, 2)]
X_ORDER = [0] + [v for s in range(1, NZ // 2) for v in (s, NZ - s)] + [NZ // 2]


def nt_dot(a, b):
    return lax.dot_general(a, b, (((1,), (1,)), ((), ())), preferred_element_type=F32)


def remote(src, dst, send, recv, device):
    return pltpu.make_async_remote_copy(
        src_ref=src, dst_ref=dst, send_sem=send, recv_sem=recv, device_id=device, device_id_type=MESH
    )


def layer_kernel(
    tokens, wq, wk, wv, wo, mixed, lse_out,
    tok, w3, wox, halo, qf, kvf, oa, ma, la, att, lse_rows, att_b, att_x, part, part_b, part_x,
    bias_a, bias_b,
    load_sem, out_sem, oy_r, zr, or_, yr, yd, xr, xd, hr, ar, cr,
):
    z, y, x, c = (lax.axis_index(n) for n in ("z", "y", "x", "c"))
    sp = z * NY + y
    shard, lanes = wk.shape
    rows = tokens.shape[0]
    loads = [
        pltpu.make_async_copy(wk, w3.at[sp, :, pl.ds(0, lanes)], load_sem.at[1]),
        pltpu.make_async_copy(wv, w3.at[sp, :, pl.ds(lanes, lanes)], load_sem.at[2]),
        pltpu.make_async_copy(wq, w3.at[sp, :, pl.ds(2 * lanes, lanes)], load_sem.at[3]),
        pltpu.make_async_copy(wo, wox.at[0, sp], load_sem.at[4]),
    ]
    for cp in loads:
        cp.start()
    copy_tokens = pltpu.make_async_copy(tokens, tok, load_sem.at[0])
    copy_tokens.start()

    def at_z(d):
        return lax.rem(z + d + NZ, NZ)

    def at_y(d):
        return lax.rem(y + d + NY, NY)

    def at_x(d):
        return lax.rem(x + d + NX, NX)

    barrier = pltpu.get_barrier_semaphore()
    peers = [{"z": at_z(1)}, {"z": at_z(-1)}]
    peers += [{"y": at_y(d)} for d in range(1, NY)]
    peers += [{"x": at_x(d)} for d in range(1, NX)]
    peers += [{"c": 1 - c}]
    for peer in peers:
        pl.semaphore_signal(barrier, inc=1, device_id=peer, device_id_type=MESH)
    for cp in loads:
        cp.wait()
    pl.semaphore_wait(barrier, len(peers))

    z_to = [{"z": at_z(1)}, {"z": at_z(-1)}]
    y_to = [{"y": at_y(1)}, {"y": at_y(-1)}]
    last = NZ // 2

    def z_parts(way, s):
        if s < last:
            return Z_PARTS
        return LAST_PARTS[way]

    def z_copy(way, s, part_):
        src = at_z(-s if way == 0 else s)
        lo, n = part_
        ref = w3.at[src * NY + y, :, pl.ds(lo * lanes, n * lanes)]
        return remote(ref, ref, out_sem.at[0], zr.at[way, s - 1, lo // 2], z_to[way])

    def z_send(way, s, part_):
        src = at_z(-(s - 1) if way == 0 else s - 1)
        lo, n = part_
        ref = w3.at[src * NY + y, :, pl.ds(lo * lanes, n * lanes)]
        remote(ref, ref, out_sem.at[0], zr.at[way, s - 1, lo // 2], z_to[way]).start()

    def o_parts(way, s):
        if s < last:
            return O_PARTS
        return [(2 * way, 2)]

    def o_ref(way, hop, part_):
        src = at_z(-hop if way == 0 else hop)
        lo, n = part_
        return wox.at[0, pl.ds(src * NY + lo, n)]

    def o_copy(way, s, hop, part_):
        ref = o_ref(way, hop, part_)
        lo = part_[0]
        return remote(ref, ref, out_sem.at[1], or_.at[way, s - 1, lo // 2], z_to[way])

    def y_copy(kind, slot, col):
        ref = w3.at[at_z(-slot) * NY + at_y(col)]
        split = (2 - slot % 2) * lanes
        if kind == 2:
            ref = ref.at[:, pl.ds(0, split)]
        if kind == 3:
            ref = ref.at[:, pl.ds(split, 3 * lanes - split)]
        return remote(ref, ref, out_sem.at[2], yr.at[kind, slot] if kind < 2 else yd, y_to[kind % 2])

    def y_send(slot):
        y_copy(0, slot, 0).start()
        y_copy(1, slot, 0).start()

    def y_relay(slot):
        y_copy(0, slot, -1).wait_recv()
        y_copy(2, slot, -1).start()
        y_copy(1, slot, 1).wait_recv()
        y_copy(3, slot, 1).start()

    def arrived_all(ref, sem):
        remote(ref, ref, out_sem.at[0], sem, z_to[0]).wait_recv()

    def left_all(ref, sem):
        remote(ref, ref, sem, yd, z_to[0]).wait_send()

    def x_copy(kind, slot):
        span = pl.ds(at_z(-slot) * NY, NY)
        way = (0, 1, slot % 2)[kind]
        src = wox.at[(0, 0, (NX - 1, 1)[way])[kind], span]
        dst = wox.at[(NX - 1, 1, 2)[kind], span]
        return remote(src, dst, out_sem.at[3], xr.at[kind, X_ORDER.index(slot) // 8] if kind < 2 else xd, {"x": at_x(1 if way == 0 else -1)})

    def x_send(slot):
        x_copy(0, slot).start()
        x_copy(1, slot).start()

    def x_relay(group):
        for kind in (0, 1):
            arrived_all(wox.at[0, pl.ds(0, 8 * NY)], xr.at[kind, group])
        for slot in X_ORDER[8 * group:8 * group + 8]:
            x_copy(2, slot).start()

    def o_row(d, col):
        ref = wox.at[0, z * NY + at_y(col)]
        return remote(ref, ref, out_sem.at[4], oy_r, {"y": at_y(d)})

    for d in (1, 3, 2):
        o_row(d, 0).start()
    for part_ in Z_PARTS:
        for way in (0, 1):
            z_send(way, 1, part_)
    y_send(0)
    arrived_all(wox.at[0, pl.ds(0, NY - 1)], oy_r)
    for part_ in O_PARTS:
        for way in (0, 1):
            o_copy(way, 1, 0, part_).start()
    x_send(0)
    waiting = [0]
    for s in range(1, last + 1):
        for i in range(len(Z_PARTS)):
            for way in (0, 1):
                here = z_parts(way, s)
                if i < len(here):
                    z_copy(way, s, here[i]).wait_recv()
                    if s + 1 < last or (s + 1 == last and here[i] in LAST_PARTS[way]):
                        z_send(way, s + 1, here[i])
        arrived = [s, NZ - s] if s < last else [s]
        for slot in arrived:
            y_send(slot)
        for i in range(len(O_PARTS)):
            for way in (0, 1):
                here = o_parts(way, s)
                if i < len(here):
                    o_copy(way, s, s, here[i]).wait_recv()
                    if s + 1 < last or (s + 1 == last and here[i] in [(2 * way, 2)]):
                        o_copy(way, s + 1, s, here[i]).start()
        for slot in arrived:
            x_send(slot)
        for slot in waiting:
            y_relay(slot)
        waiting = arrived
    for slot in waiting:
        y_relay(slot)
    arrived_all(w3.at[pl.ds(0, NZ)], yd)

    copy_tokens.wait()
    qkv = jnp.dot(tok[...], w3[...].reshape(NZ * NY * shard, 3 * lanes), preferred_element_type=F32)
    for j in range(2):
        side = slice(j * lanes, (j + 1) * lanes)
        kvf[j, WINDOW:, :] = qkv[:, side]
        for e in range(4):
            for b in range(4):
                picked = kvf[j, pl.ds(WINDOW + 4 * b + e, 32, stride=16), :]
                halo[e, 0, 32 * b:32 * b + 32, side] = picked.astype(BF16)
    qf[...] = qkv[:, 2 * lanes:].astype(BF16).astype(F32) * (HEAD ** -0.5)
    def prev_copy(e):
        return remote(halo.at[e, 0], halo.at[e, 4], out_sem.at[5], hr.at[0, e], z_to[0])

    def row_copy(e, k, src):
        return remote(halo.at[e, src], halo.at[e, k], out_sem.at[5], hr.at[k, e], {"y": at_y(k)})

    for e in range(4):
        prev_copy(e).start()
    for k in (1, 3, 2):
        @pl.when(y + k < NY)
        def _():
            for e in range(4):
                row_copy(e, k, 0).start()

    r = lax.broadcasted_iota(jnp.int32, (WINDOW, 2 * WINDOW), 0)
    k_ = lax.broadcasted_iota(jnp.int32, (WINDOW, 2 * WINDOW), 1)
    dist = WINDOW + r - k_
    near = (dist >= 0) & (dist <= WINDOW)
    bias_a[1] = jnp.where(near, 0.0, NEG)
    bias_a[0] = jnp.where(near & ((k_ >= WINDOW) | (sp > 0)), 0.0, NEG)
    r = lax.broadcasted_iota(jnp.int32, (WINDOW, 5 * WINDOW), 0)
    k_ = lax.broadcasted_iota(jnp.int32, (WINDOW, 5 * WINDOW), 1)
    back = lax.shift_right_logical(k_, 7)
    kr = k_ & 127
    db = lax.shift_right_logical(r, 5) - lax.shift_right_logical(kr, 5)
    dist = rows * back + 16 * ((r & 31) - (kr & 31)) + 4 * db
    seen = (dist >= 0) & (back <= sp)
    in16 = seen & (db == 0) & (dist <= 16 * WINDOW)
    in4 = seen & (dist <= 4 * WINDOW)
    bias_b[...] = jnp.where(in16 & in4, LN2, jnp.where(in16 | in4, 0.0, NEG))

    x_relay(0)
    for e in range(4):
        prev_copy(e).wait_recv()
        for k in (1, 3, 2):
            @pl.when(y + k >= NY)
            def _():
                row_copy(e, k, 4).start()

    head0 = lax.broadcasted_iota(jnp.int32, (WINDOW, lanes), 1) < HEAD

    def attend(qb, kb, vb, bias):
        q0 = jnp.where(head0, qb, 0.0).astype(BF16)
        q1 = jnp.where(head0, 0.0, qb).astype(BF16)
        s = nt_dot(jnp.concatenate([q0, q1], 0), kb)
        probs, tops, sums = [], [], []
        for h in range(2):
            sh = s[h * WINDOW:(h + 1) * WINDOW] + bias
            top = jnp.max(sh, axis=1, keepdims=True)
            w = jnp.exp(sh - top)
            tops.append(top)
            sums.append(jnp.sum(w, axis=1, keepdims=True))
            probs.append(w.astype(BF16))
        o = jnp.dot(jnp.concatenate(probs, 0), vb, preferred_element_type=F32)
        out = jnp.where(head0, o[0:WINDOW], o[WINDOW:])
        return out, jnp.where(head0, tops[0], tops[1]), jnp.where(head0, sums[0], sums[1])

    for e in range(4):
        row_copy(e, 1, 0).wait_recv()
    for e in range(4):
        for b in range(4):
            for j in range(2):
                tail = halo[e, 1, 32 * b + 24:32 * b + 32, j * lanes:(j + 1) * lanes]
                kvf[j, pl.ds(4 * b + e, 8, stride=16), :] = tail.astype(F32)
    for i in range(rows // WINDOW):
        span = slice(i * WINDOW, (i + 1) * WINDOW)
        keys = slice(i * WINDOW, (i + 2) * WINDOW)
        out, top, total = attend(
            qf[span, :], kvf[0, keys, :].astype(BF16), kvf[1, keys, :].astype(BF16), bias_a[min(i, 1)]
        )
        oa[span, :] = out
        ma[span, :] = top
        la[span, :] = total

    x_relay(1)

    for e in range(4):
        row_copy(e, 3, 0).wait_recv()
        row_copy(e, 2, 0).wait_recv()
        pick = [pl.ds(4 * b + e, 32, stride=16) for b in range(4)]
        qb = jnp.concatenate([qf[p, :] for p in pick], 0)
        kvb = halo[e].reshape(5 * WINDOW, 2 * lanes)
        out, top, total = attend(qb, kvb[:, 0:lanes], kvb[:, lanes:], bias_b[...])
        o_a = jnp.concatenate([oa[p, :] for p in pick], 0)
        m_a = jnp.concatenate([ma[p, :] for p in pick], 0)
        l_a = jnp.concatenate([la[p, :] for p in pick], 0)
        peak = jnp.maximum(top, m_a)
        f_b = jnp.exp(top - peak)
        f_a = jnp.exp(m_a - peak)
        denom = f_a * l_a + f_b * total
        res = (f_a * o_a + f_b * out) / denom
        lse = peak + jnp.log(denom)
        for b in range(4):
            att[pick[b], :] = res[32 * b:32 * b + 32]
            lse_rows[pick[b], :] = lse[32 * b:32 * b + 32]

    att_b[...] = att[...].reshape(NX, rows // NX, lanes).astype(BF16)

    def att_copy(d):
        return remote(att_b.at[at_x(d)], att_x.at[NX - d], out_sem.at[6], ar, {"x": at_x(d)})

    for d in (1, 3, 2):
        att_copy(d).start()
    att_x[0] = att_b[x]
    lse_t = lse_rows[...].T
    lse_out[0:1, :] = lse_t[0:1, :]
    lse_out[1:2, :] = lse_t[HEAD:HEAD + 1, :]
    arrived_all(wox.at[2], xd)
    arrived_all(att_x.at[pl.ds(1, NX - 1)], ar)

    groups = 8
    width = NZ * NY // groups
    hrows = rows // NX // 2

    def core_copy(j):
        return remote(part_b.at[j, 1 - c], part_x.at[j], out_sem.at[7], cr.at[j], {"c": 1 - c})

    for g in range(groups):
        span = slice(g * width, (g + 1) * width)
        acc = nt_dot(att_x[0], wox[0, span].reshape(width * shard, lanes))
        for k in range(1, NX):
            acc += nt_dot(att_x[k], wox[k, span].reshape(width * shard, lanes))
        acc = acc.reshape(2, hrows, width * shard)
        part[g] = acc
        part_b[g] = acc.astype(BF16)
        core_copy(g).start()
    for g in range(groups):
        core_copy(g).wait_recv()
        mixed[:, g * width * shard:(g + 1) * width * shard] = (part[g, c] + part_x[g].astype(F32)).astype(BF16)

    left_all(w3.at[pl.ds(0, NZ - 1)], out_sem.at[0])
    left_all(wox.at[0, pl.ds(0, (NZ - 1) * NY)], out_sem.at[1])
    left_all(w3.at[pl.ds(0, 3 * NZ)], out_sem.at[2])
    left_all(wox.at[pl.ds(0, NX - 1)], out_sem.at[3])
    left_all(wox.at[0, pl.ds(0, NY - 1)], out_sem.at[4])
    left_all(halo.at[:, pl.ds(0, 4)], out_sem.at[5])
    left_all(att_x.at[pl.ds(1, NX - 1)], out_sem.at[6])
    left_all(part_x, out_sem.at[7])


def shards(tokens, w_query, w_key, w_value, w_out):
    rows, depth = tokens.shape
    shard, lanes = w_query.shape
    n_sp = NZ * NY
    groups = 8
    wide = n_sp // groups * shard
    vmem = pl.BlockSpec(memory_space=pltpu.VMEM)
    dma = pltpu.SemaphoreType.DMA
    return pl.pallas_call(
        layer_kernel,
        name="layer",
        out_shape=(
            jax.ShapeDtypeStruct((rows // 8, depth), BF16),
            jax.ShapeDtypeStruct((2, rows), F32),
        ),
        in_specs=[pl.BlockSpec(memory_space=pl.ANY)] * 5,
        out_specs=(vmem, vmem),
        scratch_shapes=[
            pltpu.VMEM((rows, depth), BF16),
            pltpu.VMEM((n_sp, shard, 3 * lanes), BF16),
            pltpu.VMEM((NX, n_sp, shard, lanes), BF16),
            pltpu.VMEM((4, 5, WINDOW, 2 * lanes), BF16),
            pltpu.VMEM((rows, lanes), F32),
            pltpu.VMEM((2, WINDOW + rows, lanes), F32),
            pltpu.VMEM((rows, lanes), F32),
            pltpu.VMEM((rows, lanes), F32),
            pltpu.VMEM((rows, lanes), F32),
            pltpu.VMEM((rows, lanes), F32),
            pltpu.VMEM((rows, lanes), F32),
            pltpu.VMEM((NX, rows // NX, lanes), BF16),
            pltpu.VMEM((NX, rows // NX, lanes), BF16),
            pltpu.VMEM((groups, 2, rows // NX // 2, wide), F32),
            pltpu.VMEM((groups, 2, rows // NX // 2, wide), BF16),
            pltpu.VMEM((groups, rows // NX // 2, wide), BF16),
            pltpu.VMEM((2, WINDOW, 2 * WINDOW), F32),
            pltpu.VMEM((WINDOW, 5 * WINDOW), F32),
            dma((5,)),
            dma((8,)),
            dma,
            dma((2, NZ // 2, 2)),
            dma((2, NZ // 2, 2)),
            dma((2, NZ)),
            dma,
            dma((2, 2)),
            dma,
            dma((4, 4)),
            dma,
            dma((groups,)),
        ],
        compiler_params=pltpu.CompilerParams(
            collective_id=0, has_side_effects=True, vmem_limit_bytes=60 * 1024 * 1024
        ),
    )(tokens, w_query, w_key, w_value, w_out.T)


def solution(mesh):
    torus = Mesh(mesh.devices.reshape(NZ, NY, NX, 2), ("z", "y", "x", "c"))
    in_specs = (P(SP, None), P(SP, TP), P(SP, TP), P(SP, TP), P(TP, SP))
    out_specs = (P(SP + TP, None), P(TP, SP))
    return jax.shard_map(
        shards, mesh=torus, in_specs=in_specs, out_specs=out_specs, check_vma=False
    )
```

```python
import jax
import jax.numpy as jnp
from jax import lax
from jax.experimental import pallas as pl
from jax.experimental.pallas import tpu as pltpu
from jax.sharding import Mesh
from jax.sharding import PartitionSpec as P

HEAD = 64
WINDOW = 128
NZ = 16
NY = 4
NX = 4
MESH = pl.DeviceIdType.MESH
SP = ("z", "y")
TP = ("x", "c")
NEG = -1e30
LN2 = 0.6931471805599453
F32 = jnp.float32
BF16 = jnp.bfloat16
X_ORDER = [0] + [v for s in range(1, NZ // 2) for v in (s, NZ - s)] + [NZ // 2]


Q_LAG = 4
DIRECT = (NZ // 2 - 1, NZ // 2, NZ // 2 + 1)


def nt_dot(a, b):
    return lax.dot_general(a, b, (((1,), (1,)), ((), ())), preferred_element_type=F32)


def remote(src, dst, send, recv, device):
    return pltpu.make_async_remote_copy(
        src_ref=src, dst_ref=dst, send_sem=send, recv_sem=recv, device_id=device, device_id_type=MESH
    )


def layer_kernel(
    tokens, wq, wk_in, wv, wo, mixed, lse_out,
    tok, wz, wog, wox, halo, qf, kvf, oa, ma, la, att, lse_rows, att_b, att_x, part, part_b, part_x,
    bias_a, bias_b,
    load_sem, out_sem, row_r, zr, yr, yd, push_r, o_r, xr, xd, hr, ar, cr,
):
    z, y, x, c = (lax.axis_index(n) for n in ("z", "y", "x", "c"))
    sp = z * NY + y
    shard, lanes = wk_in.shape
    rows = tokens.shape[0]
    other = pl.ds(0, 2 * lanes)
    mine = pl.ds(2 * lanes, 2 * lanes)

    def load(src, dst, k):
        return pltpu.make_async_copy(src, dst, load_sem.at[k])

    def loads(first):
        lo, slot = (0, 1) if first else (2 * lanes, 0)
        return [
            load(wk_in, wz.at[sp, :, pl.ds(lo, lanes)], 1),
            load(wv, wz.at[sp, :, pl.ds(lo + lanes, lanes)], 2),
            load(wo, wog.at[slot, sp], 3),
            load(wq, wog.at[slot + 2, sp], 4),
        ]

    for core in (0, 1):
        @pl.when(c == core)
        def _():
            for cp in loads(core == 0):
                cp.start()
    copy_tokens = load(tokens, tok, 0)
    copy_tokens.start()

    def at_z(d):
        return lax.rem(z + d + NZ, NZ)

    def at_y(d):
        return lax.rem(y + d + NY, NY)

    def at_x(d):
        return lax.rem(x + d + NX, NX)

    barrier = pltpu.get_barrier_semaphore()
    peers = [{"z": at_z(1)}, {"z": at_z(-1)}]
    peers += [{"y": at_y(d)} for d in range(1, NY)]
    peers += [{"x": at_x(d)} for d in range(1, NX)]
    peers += [{"c": 1 - c}]
    for peer in peers:
        pl.semaphore_signal(barrier, inc=1, device_id=peer, device_id_type=MESH)
    r = lax.broadcasted_iota(jnp.int32, (WINDOW, 2 * WINDOW), 0)
    k_ = lax.broadcasted_iota(jnp.int32, (WINDOW, 2 * WINDOW), 1)
    dist = WINDOW + r - k_
    near = (dist >= 0) & (dist <= WINDOW)
    bias_a[1] = jnp.where(near, 0.0, NEG)
    bias_a[0] = jnp.where(near & ((k_ >= WINDOW) | (sp > 0)), 0.0, NEG)
    r = lax.broadcasted_iota(jnp.int32, (WINDOW, 5 * WINDOW), 0)
    k_ = lax.broadcasted_iota(jnp.int32, (WINDOW, 5 * WINDOW), 1)
    back = lax.shift_right_logical(k_, 7)
    kr = k_ & 127
    db = lax.shift_right_logical(r, 5) - lax.shift_right_logical(kr, 5)
    dist = rows * back + 16 * ((r & 31) - (kr & 31)) + 4 * db
    seen = (dist >= 0) & (back <= sp)
    in16 = seen & (db == 0) & (dist <= 16 * WINDOW)
    in4 = seen & (dist <= 4 * WINDOW)
    bias_b[...] = jnp.where(in16 & in4, LN2, jnp.where(in16 | in4, 0.0, NEG))

    for cp in loads(True):
        cp.wait()
    pl.semaphore_wait(barrier, len(peers))

    z_to = [{"z": at_z(1)}, {"z": at_z(-1)}]
    y_to = [{"y": at_y(1)}, {"y": at_y(-1)}]
    partner = {"c": 1 - c}
    last = NZ // 2

    def arrived_all(ref, sem):
        remote(ref, ref, out_sem.at[0], sem, z_to[0]).wait_recv()

    def left_all(ref, sem):
        remote(ref, ref, sem, xd, z_to[0]).wait_send()

    def z_ref(flow, src, way, s):
        if flow < 2:
            lo, n = (2 * flow, 2) if s < last else (2 * flow + way, 1)
            return wz.at[src * NY + y, :, pl.ds(lo * lanes, n * lanes)]
        cols = pl.ds(src * NY, NY) if s < last else pl.ds(src * NY + 2 * way, 2)
        return wog.at[flow - 2, cols]

    def z_copy(flow, way, s, hop):
        ref = z_ref(flow, at_z(-hop if way == 0 else hop), way, s)
        return remote(ref, ref, out_sem.at[flow // 2], zr.at[flow, way, s - 1], z_to[way])

    def z_first(flow):
        for way in (0, 1):
            z_copy(flow, way, 1, 0).start()

    def z_hop(flow, s):
        for way in (0, 1):
            z_copy(flow, way, s, s).wait_recv()
            if s < last:
                z_copy(flow, way, s + 1, s).start()

    def y_copy(kind, slot, col):
        ref = wz.at[at_z(-slot) * NY + at_y(col)]
        split = 2 * lanes
        if kind == 2:
            ref = ref.at[:, pl.ds(0, split)]
        if kind == 3:
            ref = ref.at[:, pl.ds(split, 2 * lanes)]
        to = {"y": at_y(2)} if kind == 4 else y_to[kind % 2]
        return remote(ref, ref, out_sem.at[3], yr.at[kind, slot] if kind < 2 else yd.at[slot], to)

    def y_send(slot):
        y_copy(0, slot, 0).start()
        y_copy(1, slot, 0).start()
        if slot in DIRECT:
            y_copy(4, slot, 0).start()

    def y_relay(slot):
        y_copy(0, slot, -1).wait_recv()
        if slot not in DIRECT:
            y_copy(2, slot, -1).start()
        y_copy(1, slot, 1).wait_recv()
        if slot not in DIRECT:
            y_copy(3, slot, 1).start()

    def y_done(slot):
        y_copy(4, slot, 2).wait_recv()
        row = pl.ds(at_z(-slot) * NY, NY)
        remote(wz.at[row, :, other], wz.at[row, :, mine], out_sem.at[4], push_r.at[0], partner).start()

    def o_push(slot):
        row = pl.ds(at_z(-slot) * NY, NY)
        group = X_ORDER.index(slot) // 4
        remote(wog.at[1, row], wog.at[0, row], out_sem.at[5], o_r.at[group], partner).start()

    def q_push(slot):
        row = pl.ds(at_z(-slot) * NY, NY)
        remote(wog.at[3, row], wog.at[2, row], out_sem.at[6], push_r.at[1], partner).start()

    def q_hop(s):
        for flow in (4, 5):
            z_hop(flow, s)
        for slot in arrived(s):
            q_push(slot)

    def arrived(s):
        if s == 0:
            return [0]
        return [s, NZ - s] if s < last else [s]

    def x_copy(kind, slot):
        span = pl.ds(at_z(-slot) * NY, NY)
        way = (0, 1, slot % 2)[kind]
        src = wox.at[(2, 0)[way], span] if kind == 2 else wog.at[0, span]
        dst = wox.at[(2, 0, 1)[kind], span]
        return remote(
            src, dst, out_sem.at[7], xr.at[kind, X_ORDER.index(slot) // 8] if kind < 2 else xd,
            {"x": at_x(1 if way == 0 else -1)},
        )

    def x_send(slot):
        x_copy(0, slot).start()
        x_copy(1, slot).start()

    def x_relay(group):
        for kind in (0, 1):
            arrived_all(wox.at[0, pl.ds(0, 8 * NY)], xr.at[kind, group])
        for slot in X_ORDER[8 * group:8 * group + 8]:
            x_copy(2, slot).start()

    def row_send(item, d):
        ref = wog.at[item, sp]
        return remote(ref, ref, out_sem.at[8], row_r.at[item], {"y": at_y(d)})

    @pl.when(c == 0)
    def _():
        remote(wog.at[1, sp], wog.at[1, sp], out_sem.at[1], push_r.at[1], partner).start()
        remote(wz.at[sp, :, other], wz.at[sp, :, other], out_sem.at[0], push_r.at[0], partner).start()
        remote(wog.at[3, sp], wog.at[3, sp], out_sem.at[2], push_r.at[2], partner).start()
        for group in range(4):
            arrived_all(wog.at[0, pl.ds(0, 4 * NY)], o_r.at[group])
            for slot in X_ORDER[4 * group:4 * group + 4]:
                x_send(slot)
        arrived_all(wz.at[:, :, mine], push_r.at[0])

    @pl.when(c == 1)
    def _():
        z_first(1)
        for d in (1, 3, 2):
            row_send(0, d).start()
        arrived_all(wog.at[1, sp], push_r.at[1])
        for d in (1, 3, 2):
            row_send(1, d).start()
        arrived_all(wz.at[sp, :, other], push_r.at[0])
        z_first(0)
        y_send(0)
        arrived_all(wog.at[3, sp], push_r.at[2])
        for item in (2, 3):
            for d in (1, 3, 2):
                row_send(item, d).start()
        for s in range(1, last + 2):
            if s <= last:
                for flow in (1, 0):
                    z_hop(flow, s)
                for slot in arrived(s):
                    y_send(slot)
            for item in (0, 1):
                if s == 1:
                    arrived_all(wog.at[0, pl.ds(0, NY - 1)], row_r.at[item])
                    z_first(2 + item)
                else:
                    z_hop(2 + item, s - 1)
            for slot in arrived(s - 1):
                x_send(slot)
                o_push(slot)
            if s == Q_LAG:
                for item in (2, 3):
                    arrived_all(wog.at[0, pl.ds(0, NY - 1)], row_r.at[item])
                    z_first(2 + item)
                q_push(0)
            if s > Q_LAG:
                q_hop(s - Q_LAG)
            for slot in arrived(s - 1):
                y_relay(slot)
            if s > 1:
                for slot in arrived(s - 2):
                    y_done(slot)
        for slot in arrived(last):
            y_done(slot)

    copy_tokens.wait()
    depth = NZ * NY * shard
    kv = jnp.dot(tok[...], wz[:, :, 2 * lanes:].reshape(depth, 2 * lanes), preferred_element_type=F32)
    for j in range(2):
        side = slice(j * lanes, (j + 1) * lanes)
        kvf[j, WINDOW:, :] = kv[:, side]
        for e in range(4):
            for b in range(4):
                picked = kvf[j, pl.ds(WINDOW + 4 * b + e, 32, stride=16), :]
                halo[e, 0, 32 * b:32 * b + 32, side] = picked.astype(BF16)

    def prev_copy(e):
        return remote(halo.at[e, 0], halo.at[e, 4], out_sem.at[9], hr.at[0, e], z_to[0])

    def row_copy(e, k, src):
        return remote(halo.at[e, src], halo.at[e, k], out_sem.at[9], hr.at[k, e], {"y": at_y(k)})

    def relay_copy(e, k):
        return remote(halo.at[e, k], halo.at[e, 2], out_sem.at[12], hr.at[2, e], y_to[0 if k == 1 else 1])

    def q_next(s):
        @pl.when(c == 1)
        def _():
            q_hop(s)

    for e in range(4):
        prev_copy(e).start()
        for k in (1, 3):
            @pl.when(y + k < NY)
            def _():
                row_copy(e, k, 0).start()

    def wrap(e):
        prev_copy(e).wait_recv()
        for k in (1, 3):
            @pl.when(y + k >= NY)
            def _():
                row_copy(e, k, 4).start()

    def pass_on(e):
        row_copy(e, 1, 0).wait_recv()

        @pl.when((y == 2) | ((y < 2) & (e < 2)))
        def _():
            relay_copy(e, 1).start()

        row_copy(e, 3, 0).wait_recv()

        @pl.when((y == 1) | ((y >= 2) & (e >= 2)))
        def _():
            relay_copy(e, 3).start()

    done = last + 1 - Q_LAG
    q_next(done + 1)
    wrap(0)
    wrap(1)
    for s in range(done + 2, last):
        q_next(s)
    wrap(2)
    wrap(3)
    q_next(last)
    x_relay(0)
    pass_on(0)
    pass_on(1)

    @pl.when(c == 0)
    def _():
        arrived_all(wog.at[2], push_r.at[1])

    q = jnp.dot(tok[...], wog[2].reshape(depth, lanes), preferred_element_type=F32)
    qf[...] = q.astype(BF16).astype(F32) * (HEAD ** -0.5)
    pass_on(2)
    pass_on(3)

    head0 = lax.broadcasted_iota(jnp.int32, (WINDOW, lanes), 1) < HEAD

    def attend(qb, kb, vb, bias):
        q0 = jnp.where(head0, qb, 0.0).astype(BF16)
        q1 = jnp.where(head0, 0.0, qb).astype(BF16)
        s = nt_dot(jnp.concatenate([q0, q1], 0), kb)
        probs, tops, sums = [], [], []
        for h in range(2):
            sh = s[h * WINDOW:(h + 1) * WINDOW] + bias
            top = jnp.max(sh, axis=1, keepdims=True)
            w = jnp.exp(sh - top)
            tops.append(top)
            sums.append(jnp.sum(w, axis=1, keepdims=True))
            probs.append(w.astype(BF16))
        o = jnp.dot(jnp.concatenate(probs, 0), vb, preferred_element_type=F32)
        out = jnp.where(head0, o[0:WINDOW], o[WINDOW:])
        return out, jnp.where(head0, tops[0], tops[1]), jnp.where(head0, sums[0], sums[1])

    for e in range(4):
        for b in range(4):
            for j in range(2):
                tail = halo[e, 1, 32 * b + 24:32 * b + 32, j * lanes:(j + 1) * lanes]
                kvf[j, pl.ds(4 * b + e, 8, stride=16), :] = tail.astype(F32)
    for i in range(rows // WINDOW):
        span = slice(i * WINDOW, (i + 1) * WINDOW)
        keys = slice(i * WINDOW, (i + 2) * WINDOW)
        out, top, total = attend(
            qf[span, :], kvf[0, keys, :].astype(BF16), kvf[1, keys, :].astype(BF16), bias_a[min(i, 1)]
        )
        oa[span, :] = out
        ma[span, :] = top
        la[span, :] = total

    x_relay(1)

    for e in range(4):
        row_copy(e, 2, 0).wait_recv()
        pick = [pl.ds(4 * b + e, 32, stride=16) for b in range(4)]
        qb = jnp.concatenate([qf[p, :] for p in pick], 0)
        kvb = halo[e].reshape(5 * WINDOW, 2 * lanes)
        out, top, total = attend(qb, kvb[:, 0:lanes], kvb[:, lanes:], bias_b[...])
        o_a = jnp.concatenate([oa[p, :] for p in pick], 0)
        m_a = jnp.concatenate([ma[p, :] for p in pick], 0)
        l_a = jnp.concatenate([la[p, :] for p in pick], 0)
        peak = jnp.maximum(top, m_a)
        f_b = jnp.exp(top - peak)
        f_a = jnp.exp(m_a - peak)
        denom = f_a * l_a + f_b * total
        res = (f_a * o_a + f_b * out) / denom
        lse = peak + jnp.log(denom)
        for b in range(4):
            att[pick[b], :] = res[32 * b:32 * b + 32]
            lse_rows[pick[b], :] = lse[32 * b:32 * b + 32]

    att_b[...] = att[...].reshape(NX, rows // NX, lanes).astype(BF16)

    def att_copy(d):
        return remote(att_b.at[at_x(d)], att_x.at[NX - d], out_sem.at[10], ar, {"x": at_x(d)})

    for d in (1, 3, 2):
        att_copy(d).start()
    att_x[0] = att_b[x]
    lse_t = lse_rows[...].T
    lse_out[0:1, :] = lse_t[0:1, :]
    lse_out[1:2, :] = lse_t[HEAD:HEAD + 1, :]
    arrived_all(wox.at[1], xd)
    arrived_all(att_x.at[pl.ds(1, NX - 1)], ar)

    groups = 8
    width = NZ * NY // groups
    hrows = rows // NX // 2

    def core_copy(j):
        return remote(part_b.at[j, 1 - c], part_x.at[j], out_sem.at[11], cr.at[j], {"c": 1 - c})

    for g in range(groups):
        span = slice(g * width, (g + 1) * width)
        acc = nt_dot(att_x[0], wog[0, span].reshape(width * shard, lanes))
        for k in range(1, NX):
            acc += nt_dot(att_x[k], wox[k - 1, span].reshape(width * shard, lanes))
        acc = acc.reshape(2, hrows, width * shard)
        part[g] = acc
        part_b[g] = acc.astype(BF16)
        core_copy(g).start()
    for g in range(groups):
        core_copy(g).wait_recv()
        mixed[:, g * width * shard:(g + 1) * width * shard] = (part[g, c] + part_x[g].astype(F32)).astype(BF16)

    @pl.when(c == 0)
    def _():
        left_all(wz.at[sp, :, other], out_sem.at[0])
        left_all(wog.at[1, sp], out_sem.at[1])
        left_all(wog.at[3, sp], out_sem.at[2])

    @pl.when(c == 1)
    def _():
        left_all(wz.at[pl.ds(0, NZ - 1)], out_sem.at[0])
        for k in (1, 2):
            left_all(wog.at[pl.ds(0, 2), pl.ds(0, (NZ - 1) * NY)], out_sem.at[k])
        left_all(wz.at[pl.ds(0, 3 * NZ)], out_sem.at[3])
        left_all(wz.at[:, :, mine], out_sem.at[4])
        for k in (5, 6):
            left_all(wog.at[0], out_sem.at[k])
        left_all(wog.at[:, pl.ds(0, NY - 1)], out_sem.at[8])

    left_all(wox, out_sem.at[7])
    left_all(halo.at[:, pl.ds(0, 3)], out_sem.at[9])
    left_all(halo.at[0, pl.ds(0, 2)], out_sem.at[12])

    @pl.when((y == 1) | (y == 2))
    def _():
        left_all(halo.at[:, 0], out_sem.at[12])

    left_all(att_x.at[pl.ds(1, NX - 1)], out_sem.at[10])
    left_all(part_x, out_sem.at[11])


def shards(tokens, w_query, w_key, w_value, w_out):
    rows, depth = tokens.shape
    shard, lanes = w_query.shape
    n_sp = NZ * NY
    groups = 8
    wide = n_sp // groups * shard
    vmem = pl.BlockSpec(memory_space=pltpu.VMEM)
    dma = pltpu.SemaphoreType.DMA
    return pl.pallas_call(
        layer_kernel,
        name="layer",
        out_shape=(
            jax.ShapeDtypeStruct((rows // 8, depth), BF16),
            jax.ShapeDtypeStruct((2, rows), F32),
        ),
        in_specs=[pl.BlockSpec(memory_space=pl.ANY)] * 5,
        out_specs=(vmem, vmem),
        scratch_shapes=[
            pltpu.VMEM((rows, depth), BF16),
            pltpu.VMEM((n_sp, shard, 4 * lanes), BF16),
            pltpu.VMEM((4, n_sp, shard, lanes), BF16),
            pltpu.VMEM((NX - 1, n_sp, shard, lanes), BF16),
            pltpu.VMEM((4, 5, WINDOW, 2 * lanes), BF16),
            pltpu.VMEM((rows, lanes), F32),
            pltpu.VMEM((2, WINDOW + rows, lanes), F32),
            pltpu.VMEM((rows, lanes), F32),
            pltpu.VMEM((rows, lanes), F32),
            pltpu.VMEM((rows, lanes), F32),
            pltpu.VMEM((rows, lanes), F32),
            pltpu.VMEM((rows, lanes), F32),
            pltpu.VMEM((NX, rows // NX, lanes), BF16),
            pltpu.VMEM((NX, rows // NX, lanes), BF16),
            pltpu.VMEM((groups, 2, rows // NX // 2, wide), F32),
            pltpu.VMEM((groups, 2, rows // NX // 2, wide), BF16),
            pltpu.VMEM((groups, rows // NX // 2, wide), BF16),
            pltpu.VMEM((2, WINDOW, 2 * WINDOW), F32),
            pltpu.VMEM((WINDOW, 5 * WINDOW), F32),
            dma((5,)),
            dma((13,)),
            dma((4,)),
            dma((6, 2, NZ // 2)),
            dma((2, NZ)),
            dma((NZ,)),
            dma((3,)),
            dma((4,)),
            dma((2, 2)),
            dma,
            dma((4, 4)),
            dma,
            dma((groups,)),
        ],
        compiler_params=pltpu.CompilerParams(
            collective_id=0, has_side_effects=True, vmem_limit_bytes=60 * 1024 * 1024
        ),
    )(tokens, w_query, w_key, w_value, w_out.T)


def solution(mesh):
    torus = Mesh(mesh.devices.reshape(NZ, NY, NX, 2), ("z", "y", "x", "c"))
    in_specs = (P(SP, None), P(SP, TP), P(SP, TP), P(SP, TP), P(TP, SP))
    out_specs = (P(SP + TP, None), P(TP, SP))
    return jax.shard_map(
        shards, mesh=torus, in_specs=in_specs, out_specs=out_specs, check_vma=False
    )
```

```python
import jax
import jax.numpy as jnp
from jax import lax
from jax.experimental import pallas as pl
from jax.experimental.pallas import tpu as pltpu
from jax.sharding import Mesh
from jax.sharding import PartitionSpec as P

HEAD = 64
WINDOW = 128
NZ = 16
NY = 4
NX = 4
MESH = pl.DeviceIdType.MESH
SP = ("z", "y")
TP = ("x", "c")
NEG = -1e30
LN2 = 0.6931471805599453
F32 = jnp.float32
BF16 = jnp.bfloat16
X_ORDER = [0] + [v for s in range(1, NZ // 2) for v in (s, NZ - s)] + [NZ // 2]


Y_LAG = 2
Y_DONE = 4
Z_FLOWS = (2, 1, 0)
DIRECT = (NZ // 2 - 1, NZ // 2, NZ // 2 + 1)


def nt_dot(a, b):
    return lax.dot_general(a, b, (((1,), (1,)), ((), ())), preferred_element_type=F32)


def remote(src, dst, send, recv, device):
    return pltpu.make_async_remote_copy(
        src_ref=src, dst_ref=dst, send_sem=send, recv_sem=recv, device_id=device, device_id_type=MESH
    )


def layer_kernel(
    tokens, wq, wk_in, wv, wo, ours, theirs, lse_out,
    tok, wz, wog, wox, halo, qf, kvf, oa, ma, la, att, lse_rows, att_b, att_x, part, part_b,
    bias_a, bias_b,
    load_sem, out_sem, row_r, zr, yr, yd, push_r, o_r, xr, xd, hr, ar, cr,
):
    z, y, x, c = (lax.axis_index(n) for n in ("z", "y", "x", "c"))
    sp = z * NY + y
    shard, lanes = wk_in.shape
    rows = tokens.shape[0]
    other = pl.ds(0, 3 * lanes)
    mine = pl.ds(3 * lanes, 3 * lanes)

    def load(src, dst, k):
        return pltpu.make_async_copy(src, dst, load_sem.at[k])

    def loads(first):
        lo, slot = (0, 1) if first else (3 * lanes, 0)
        return [
            load(wk_in, wz.at[sp, :, pl.ds(lo, lanes)], 1),
            load(wv, wz.at[sp, :, pl.ds(lo + lanes, lanes)], 2),
            load(wq, wz.at[sp, :, pl.ds(lo + 2 * lanes, lanes)], 3),
            load(wo, wog.at[slot, sp], 4),
        ]

    for core in (0, 1):
        @pl.when(c == core)
        def _():
            for cp in loads(core == 0):
                cp.start()
    copy_tokens = load(tokens, tok, 0)
    copy_tokens.start()

    def at_z(d):
        return lax.rem(z + d + NZ, NZ)

    def at_y(d):
        return lax.rem(y + d + NY, NY)

    def at_x(d):
        return lax.rem(x + d + NX, NX)

    barrier = pltpu.get_barrier_semaphore()
    peers = [{"z": at_z(1)}, {"z": at_z(-1)}]
    peers += [{"y": at_y(d)} for d in range(1, NY)]
    peers += [{"x": at_x(d)} for d in range(1, NX)]
    peers += [{"c": 1 - c}]
    for peer in peers:
        pl.semaphore_signal(barrier, inc=1, device_id=peer, device_id_type=MESH)
    r = lax.broadcasted_iota(jnp.int32, (WINDOW, 2 * WINDOW), 0)
    k_ = lax.broadcasted_iota(jnp.int32, (WINDOW, 2 * WINDOW), 1)
    dist = WINDOW + r - k_
    near = (dist >= 0) & (dist <= WINDOW)
    bias_a[1] = jnp.where(near, 0.0, NEG)
    bias_a[0] = jnp.where(near & ((k_ >= WINDOW) | (sp > 0)), 0.0, NEG)
    r = lax.broadcasted_iota(jnp.int32, (WINDOW, 5 * WINDOW), 0)
    k_ = lax.broadcasted_iota(jnp.int32, (WINDOW, 5 * WINDOW), 1)
    back = lax.shift_right_logical(k_, 7)
    kr = k_ & 127
    db = lax.shift_right_logical(r, 5) - lax.shift_right_logical(kr, 5)
    dist = rows * back + 16 * ((r & 31) - (kr & 31)) + 4 * db
    seen = (dist >= 0) & (back <= sp)
    in16 = seen & (db == 0) & (dist <= 16 * WINDOW)
    in4 = seen & (dist <= 4 * WINDOW)
    bias_b[...] = jnp.where(in16 & in4, LN2, jnp.where(in16 | in4, 0.0, NEG))

    for cp in loads(True):
        cp.wait()
    pl.semaphore_wait(barrier, len(peers))

    z_to = [{"z": at_z(1)}, {"z": at_z(-1)}]
    y_to = [{"y": at_y(1)}, {"y": at_y(-1)}]
    partner = {"c": 1 - c}
    last = NZ // 2

    def arrived_all(ref, sem):
        remote(ref, ref, out_sem.at[0], sem, z_to[0]).wait_recv()

    def left_all(ref, sem):
        remote(ref, ref, sem, xd, z_to[0]).wait_send()

    def z_ref(flow, src, way, s):
        if flow < 3:
            lo, n = (2 * flow, 2) if s < last else (2 * flow + way, 1)
            return wz.at[src * NY + y, :, pl.ds(lo * lanes, n * lanes)]
        cols = pl.ds(src * NY, NY) if s < last else pl.ds(src * NY + 2 * way, 2)
        return wog.at[flow - 3, cols]

    def z_copy(flow, way, s, hop):
        ref = z_ref(flow, at_z(-hop if way == 0 else hop), way, s)
        return remote(ref, ref, out_sem.at[flow // 3], zr.at[flow, way, s - 1], z_to[way])

    def z_first(flow):
        for way in (0, 1):
            z_copy(flow, way, 1, 0).start()

    def z_hop(flow, s):
        for way in (0, 1):
            z_copy(flow, way, s, s).wait_recv()
            if s < last:
                z_copy(flow, way, s + 1, s).start()

    def y_copy(kind, slot, col):
        ref = wz.at[at_z(-slot) * NY + at_y(col)]
        split = 3 * lanes
        if kind == 2:
            ref = ref.at[:, pl.ds(0, split)]
        if kind == 3:
            ref = ref.at[:, pl.ds(split, 3 * lanes)]
        to = {"y": at_y(2)} if kind == 4 else y_to[kind % 2]
        return remote(
            ref, ref, out_sem.at[3 if kind < 2 else 2], yr.at[kind, slot] if kind < 2 else yd.at[slot], to
        )

    def y_send(slot):
        y_copy(0, slot, 0).start()
        y_copy(1, slot, 0).start()
        if slot in DIRECT:
            y_copy(4, slot, 0).start()

    def y_relay(slot):
        y_copy(0, slot, -1).wait_recv()
        if slot not in DIRECT:
            y_copy(2, slot, -1).start()
        y_copy(1, slot, 1).wait_recv()
        if slot not in DIRECT:
            y_copy(3, slot, 1).start()

    def y_done(slot):
        y_copy(4, slot, 2).wait_recv()
        row = pl.ds(at_z(-slot) * NY, NY)
        remote(wz.at[row, :, other], wz.at[row, :, mine], out_sem.at[4], push_r.at[0], partner).start()

    def o_push(slot):
        row = pl.ds(at_z(-slot) * NY, NY)
        group = X_ORDER.index(slot) // 4
        remote(wog.at[1, row], wog.at[0, row], out_sem.at[5], o_r.at[group], partner).start()

    def arrived(s):
        if s == 0:
            return [0]
        return [s, NZ - s] if s < last else [s]

    def x_copy(kind, slot):
        span = pl.ds(at_z(-slot) * NY, NY)
        way = (0, 1, slot % 2)[kind]
        src = wox.at[(2, 0)[way], span] if kind == 2 else wog.at[0, span]
        dst = wox.at[(2, 0, 1)[kind], span]
        return remote(
            src, dst, out_sem.at[7], xr.at[kind, X_ORDER.index(slot) // 8] if kind < 2 else xd,
            {"x": at_x(1 if way == 0 else -1)},
        )

    def x_send(slot):
        x_copy(0, slot).start()
        x_copy(1, slot).start()

    def x_relay(group):
        for kind in (0, 1):
            arrived_all(wox.at[0, pl.ds(0, 8 * NY)], xr.at[kind, group])
        for slot in X_ORDER[8 * group:8 * group + 8]:
            x_copy(2, slot).start()

    def row_send(item, d):
        ref = wog.at[item, sp]
        return remote(ref, ref, out_sem.at[8], row_r.at[item], {"y": at_y(d)})

    @pl.when(c == 0)
    def _():
        remote(wz.at[sp, :, other], wz.at[sp, :, other], out_sem.at[0], push_r.at[0], partner).start()
        remote(wog.at[1, sp], wog.at[1, sp], out_sem.at[1], push_r.at[1], partner).start()
        for group in range(4):
            arrived_all(wog.at[0, pl.ds(0, 4 * NY)], o_r.at[group])
            for slot in X_ORDER[4 * group:4 * group + 4]:
                x_send(slot)
        arrived_all(wz.at[:, :, mine], push_r.at[0])

    @pl.when(c == 1)
    def _():
        z_first(2)
        for d in (1, 3, 2):
            row_send(0, d).start()
        arrived_all(wz.at[sp, :, other], push_r.at[0])
        z_first(0)
        z_first(1)
        y_send(0)
        arrived_all(wog.at[1, sp], push_r.at[1])
        for d in (1, 3, 2):
            row_send(1, d).start()
        for s in range(1, last + 2):
            if s <= last:
                for flow in Z_FLOWS:
                    z_hop(flow, s)
                for slot in arrived(s):
                    y_send(slot)
            for item in (0, 1):
                if s == 1:
                    arrived_all(wog.at[0, pl.ds(0, NY - 1)], row_r.at[item])
                    z_first(3 + item)
                else:
                    z_hop(3 + item, s - 1)
            for slot in arrived(s - 1):
                x_send(slot)
                o_push(slot)
            if s >= Y_LAG:
                for slot in arrived(s - Y_LAG):
                    y_relay(slot)
            if s >= Y_DONE:
                for slot in arrived(s - Y_DONE):
                    y_done(slot)
        for s in range(last + 2, last + Y_DONE + 1):
            if s <= last + Y_LAG:
                for slot in arrived(s - Y_LAG):
                    y_relay(slot)
            for slot in arrived(s - Y_DONE):
                y_done(slot)

    x_relay(0)
    copy_tokens.wait()
    depth = NZ * NY * shard
    qkv = jnp.dot(tok[...], wz[:, :, 3 * lanes:].reshape(depth, 3 * lanes), preferred_element_type=F32)
    for j in range(2):
        side = slice(j * lanes, (j + 1) * lanes)
        kvf[j, WINDOW:, :] = qkv[:, side]
        for e in range(4):
            for b in range(4):
                picked = kvf[j, pl.ds(WINDOW + 4 * b + e, 32, stride=16), :]
                halo[e, 0, 32 * b:32 * b + 32, side] = picked.astype(BF16)

    def prev_copy(e):
        return remote(halo.at[e, 0], halo.at[e, 4], out_sem.at[9], hr.at[0, e], z_to[0])

    def row_copy(e, k, src):
        return remote(halo.at[e, src], halo.at[e, k], out_sem.at[9], hr.at[k, e], {"y": at_y(k)})

    def relay_copy(e, k):
        return remote(halo.at[e, k], halo.at[e, 2], out_sem.at[12], hr.at[2, e], y_to[0 if k == 1 else 1])

    for e in range(4):
        prev_copy(e).start()
        for k in (1, 3):
            @pl.when(y + k < NY)
            def _():
                row_copy(e, k, 0).start()

    def wrap(e):
        prev_copy(e).wait_recv()
        for k in (1, 3):
            @pl.when(y + k >= NY)
            def _():
                row_copy(e, k, 4).start()

    def pass_on(e):
        row_copy(e, 1, 0).wait_recv()

        @pl.when((y == 2) | ((y < 2) & (e < 2)))
        def _():
            relay_copy(e, 1).start()

        row_copy(e, 3, 0).wait_recv()

        @pl.when((y == 1) | ((y >= 2) & (e >= 2)))
        def _():
            relay_copy(e, 3).start()

    qf[...] = qkv[:, 2 * lanes:].astype(BF16).astype(F32) * (HEAD ** -0.5)
    for e in range(4):
        wrap(e)
    x_relay(1)
    for e in range(4):
        pass_on(e)

    head0 = lax.broadcasted_iota(jnp.int32, (WINDOW, lanes), 1) < HEAD

    def attend(qb, kb, vb, bias):
        q0 = jnp.where(head0, qb, 0.0).astype(BF16)
        q1 = jnp.where(head0, 0.0, qb).astype(BF16)
        s = nt_dot(jnp.concatenate([q0, q1], 0), kb)
        probs, tops, sums = [], [], []
        for h in range(2):
            sh = s[h * WINDOW:(h + 1) * WINDOW] + bias
            top = jnp.max(sh, axis=1, keepdims=True)
            w = jnp.exp(sh - top)
            tops.append(top)
            sums.append(jnp.sum(w, axis=1, keepdims=True))
            probs.append(w.astype(BF16))
        o = jnp.dot(jnp.concatenate(probs, 0), vb, preferred_element_type=F32)
        out = jnp.where(head0, o[0:WINDOW], o[WINDOW:])
        return out, jnp.where(head0, tops[0], tops[1]), jnp.where(head0, sums[0], sums[1])

    for e in range(4):
        for b in range(4):
            for j in range(2):
                tail = halo[e, 1, 32 * b + 24:32 * b + 32, j * lanes:(j + 1) * lanes]
                kvf[j, pl.ds(4 * b + e, 8, stride=16), :] = tail.astype(F32)
    for i in range(rows // WINDOW):
        span = slice(i * WINDOW, (i + 1) * WINDOW)
        keys = slice(i * WINDOW, (i + 2) * WINDOW)
        out, top, total = attend(
            qf[span, :], kvf[0, keys, :].astype(BF16), kvf[1, keys, :].astype(BF16), bias_a[min(i, 1)]
        )
        oa[span, :] = out
        ma[span, :] = top
        la[span, :] = total


    for e in range(4):
        row_copy(e, 2, 0).wait_recv()
        pick = [pl.ds(4 * b + e, 32, stride=16) for b in range(4)]
        qb = jnp.concatenate([qf[p, :] for p in pick], 0)
        kvb = halo[e].reshape(5 * WINDOW, 2 * lanes)
        out, top, total = attend(qb, kvb[:, 0:lanes], kvb[:, lanes:], bias_b[...])
        o_a = jnp.concatenate([oa[p, :] for p in pick], 0)
        m_a = jnp.concatenate([ma[p, :] for p in pick], 0)
        l_a = jnp.concatenate([la[p, :] for p in pick], 0)
        peak = jnp.maximum(top, m_a)
        f_b = jnp.exp(top - peak)
        f_a = jnp.exp(m_a - peak)
        denom = f_a * l_a + f_b * total
        res = (f_a * o_a + f_b * out) / denom
        lse = peak + jnp.log(denom)
        for b in range(4):
            att[pick[b], :] = res[32 * b:32 * b + 32]
            lse_rows[pick[b], :] = lse[32 * b:32 * b + 32]

    att_b[...] = att[...].reshape(NX, rows // NX, lanes).astype(BF16)

    def att_copy(d):
        return remote(att_b.at[at_x(d)], att_x.at[NX - d], out_sem.at[10], ar, {"x": at_x(d)})

    for d in (1, 3, 2):
        att_copy(d).start()
    att_x[0] = att_b[x]
    lse_t = lse_rows[...].T
    lse_out[0:1, :] = lse_t[0:1, :]
    lse_out[1:2, :] = lse_t[HEAD:HEAD + 1, :]
    groups = 8
    width = NZ * NY // groups
    hrows = rows // NX // 2
    for g in range(groups):
        w_own = wog[0, g * width:(g + 1) * width].reshape(width * shard, lanes)
        part[g] = nt_dot(att_x[0], w_own).reshape(2, hrows, width * shard)
    arrived_all(wox.at[1], xd)
    arrived_all(att_x.at[pl.ds(1, NX - 1)], ar)

    def core_copy(j):
        return remote(part_b.at[j, 1 - c], theirs.at[j], out_sem.at[11], cr, {"c": 1 - c})

    for g in range(groups):
        span = slice(g * width, (g + 1) * width)
        acc = nt_dot(att_x[1], wox[0, span].reshape(width * shard, lanes))
        for k in range(2, NX):
            acc += nt_dot(att_x[k], wox[k - 1, span].reshape(width * shard, lanes))
        part_b[g] = (acc.reshape(2, hrows, width * shard) + part[g]).astype(BF16)
        core_copy(g).start()
    pltpu.make_async_copy(part_b.at[:, c], ours, load_sem.at[1]).start()
    remote(part_b.at[:, c], theirs, out_sem.at[11], cr, partner).wait_recv()
    pltpu.make_async_copy(part_b.at[:, c], ours, load_sem.at[1]).wait()
    @pl.when(c == 0)
    def _():
        left_all(wz.at[sp, :, other], out_sem.at[0])
        left_all(wog.at[1, sp], out_sem.at[1])

    @pl.when(c == 1)
    def _():
        left_all(wz.at[pl.ds(0, NZ - 1)], out_sem.at[0])
        left_all(wog.at[:, pl.ds(0, (NZ - 1) * NY)], out_sem.at[1])
        left_all(wz.at[pl.ds(0, 2 * NZ)], out_sem.at[3])
        left_all(wz.at[pl.ds(0, NZ)], out_sem.at[2])
        left_all(wz.at[:, :, mine], out_sem.at[4])
        left_all(wog.at[0], out_sem.at[5])
        left_all(wog.at[:, pl.ds(0, NY - 1)], out_sem.at[8])

    left_all(wox, out_sem.at[7])
    left_all(halo.at[:, pl.ds(0, 3)], out_sem.at[9])
    left_all(halo.at[0, pl.ds(0, 2)], out_sem.at[12])

    @pl.when((y == 1) | (y == 2))
    def _():
        left_all(halo.at[:, 0], out_sem.at[12])

    left_all(att_x.at[pl.ds(1, NX - 1)], out_sem.at[10])
    left_all(part_b.at[:, c], out_sem.at[11])


def sum_kernel(ours, theirs, lse, mixed, lse_out):
    wide = ours.shape[2]
    for g in range(ours.shape[0]):
        total = ours[g].astype(F32) + theirs[g].astype(F32)
        mixed[:, g * wide:(g + 1) * wide] = total.astype(BF16)
    lse_out[...] = lse[...]


def shards(tokens, w_query, w_key, w_value, w_out):
    rows, depth = tokens.shape
    shard, lanes = w_query.shape
    n_sp = NZ * NY
    groups = 8
    wide = n_sp // groups * shard
    vmem = pl.BlockSpec(memory_space=pltpu.VMEM)
    anywhere = pl.BlockSpec(memory_space=pl.ANY)
    dma = pltpu.SemaphoreType.DMA
    ours, theirs, lse = pl.pallas_call(
        layer_kernel,
        name="layer",
        out_shape=(
            jax.ShapeDtypeStruct((groups, rows // 8, wide), BF16),
            jax.ShapeDtypeStruct((groups, rows // 8, wide), BF16),
            jax.ShapeDtypeStruct((2, rows), F32),
        ),
        in_specs=[pl.BlockSpec(memory_space=pl.ANY)] * 5,
        out_specs=(anywhere, anywhere, vmem),
        scratch_shapes=[
            pltpu.VMEM((rows, depth), BF16),
            pltpu.VMEM((n_sp, shard, 6 * lanes), BF16),
            pltpu.VMEM((2, n_sp, shard, lanes), BF16),
            pltpu.VMEM((NX - 1, n_sp, shard, lanes), BF16),
            pltpu.VMEM((4, 5, WINDOW, 2 * lanes), BF16),
            pltpu.VMEM((rows, lanes), F32),
            pltpu.VMEM((2, WINDOW + rows, lanes), F32),
            pltpu.VMEM((rows, lanes), F32),
            pltpu.VMEM((rows, lanes), F32),
            pltpu.VMEM((rows, lanes), F32),
            pltpu.VMEM((rows, lanes), F32),
            pltpu.VMEM((rows, lanes), F32),
            pltpu.VMEM((NX, rows // NX, lanes), BF16),
            pltpu.VMEM((NX, rows // NX, lanes), BF16),
            pltpu.VMEM((groups, 2, rows // NX // 2, wide), F32),
            pltpu.VMEM((groups, 2, rows // NX // 2, wide), BF16),
            pltpu.VMEM((2, WINDOW, 2 * WINDOW), F32),
            pltpu.VMEM((WINDOW, 5 * WINDOW), F32),
            dma((5,)),
            dma((13,)),
            dma((2,)),
            dma((5, 2, NZ // 2)),
            dma((2, NZ)),
            dma((NZ,)),
            dma((2,)),
            dma((4,)),
            dma((2, 2)),
            dma,
            dma((4, 4)),
            dma,
            dma,
        ],
        compiler_params=pltpu.CompilerParams(
            collective_id=0, has_side_effects=True, vmem_limit_bytes=60 * 1024 * 1024
        ),
    )(tokens, w_query, w_key, w_value, w_out.T)
    return pl.pallas_call(
        sum_kernel,
        name="total",
        out_shape=(
            jax.ShapeDtypeStruct((rows // 8, depth), BF16),
            jax.ShapeDtypeStruct((2, rows), F32),
        ),
        in_specs=[vmem] * 3,
        out_specs=(vmem, vmem),
    )(ours, theirs, lse)


def solution(mesh):
    torus = Mesh(mesh.devices.reshape(NZ, NY, NX, 2), ("z", "y", "x", "c"))
    in_specs = (P(SP, None), P(SP, TP), P(SP, TP), P(SP, TP), P(TP, SP))
    out_specs = (P(SP + TP, None), P(TP, SP))
    return jax.shard_map(
        shards, mesh=torus, in_specs=in_specs, out_specs=out_specs, check_vma=False
    )
```

```python
import jax
import jax.numpy as jnp
from jax import lax
from jax.experimental import pallas as pl
from jax.experimental.pallas import tpu as pltpu
from jax.sharding import Mesh
from jax.sharding import PartitionSpec as P

HEAD = 64
WINDOW = 128
NZ = 16
NY = 4
NX = 4
MESH = pl.DeviceIdType.MESH
SP = ("z", "y")
TP = ("x", "c")
NEG = -1e30
LN2 = 0.6931471805599453
F32 = jnp.float32
BF16 = jnp.bfloat16
X_ORDER = [0] + [v for s in range(1, NZ // 2) for v in (s, NZ - s)] + [NZ // 2]


O_LAG = 1
Y_LAG = 1
Y_DONE = 3
Z_FLOWS = (2, 1, 0)
DIRECT = (NZ // 2,)


def nt_dot(a, b):
    return lax.dot_general(a, b, (((1,), (1,)), ((), ())), preferred_element_type=F32)


def remote(src, dst, send, recv, device):
    return pltpu.make_async_remote_copy(
        src_ref=src, dst_ref=dst, send_sem=send, recv_sem=recv, device_id=device, device_id_type=MESH
    )


def layer_kernel(
    tokens, wq, wk_in, wv, wo, ours, theirs, lse_out,
    tok, acc, wz, wog, wox, halo, qf, kvf, oa, ma, la, att, lse_rows, att_b, att_x, part, part_b,
    bias_a, bias_b,
    load_sem, out_sem, row_r, zr, yr, yd, push_r, o_r, xr, xd, hr, ar, cr,
):
    z, y, x, c = (lax.axis_index(n) for n in ("z", "y", "x", "c"))
    sp = z * NY + y
    shard, lanes = wk_in.shape
    rows = tokens.shape[0]
    other = pl.ds(0, 3 * lanes)
    mine = pl.ds(3 * lanes, 3 * lanes)

    def load(src, dst, k):
        return pltpu.make_async_copy(src, dst, load_sem.at[k])

    def loads(first):
        lo, slot = (0, 1) if first else (3 * lanes, 0)
        return [
            load(wk_in, wz.at[sp, :, pl.ds(lo, lanes)], 1),
            load(wv, wz.at[sp, :, pl.ds(lo + lanes, lanes)], 2),
            load(wq, wz.at[sp, :, pl.ds(lo + 2 * lanes, lanes)], 3),
            load(wo, wog.at[slot, sp], 4),
        ]

    for core in (0, 1):
        @pl.when(c == core)
        def _():
            for cp in loads(core == 0):
                cp.start()
    copy_tokens = load(tokens, tok, 0)
    copy_tokens.start()

    def at_z(d):
        return lax.rem(z + d + NZ, NZ)

    def at_y(d):
        return lax.rem(y + d + NY, NY)

    def at_x(d):
        return lax.rem(x + d + NX, NX)

    barrier = pltpu.get_barrier_semaphore()
    peers = [{"z": at_z(1)}, {"z": at_z(-1)}]
    peers += [{"y": at_y(d)} for d in range(1, NY)]
    peers += [{"x": at_x(d)} for d in range(1, NX)]
    peers += [{"c": 1 - c}]
    for peer in peers:
        pl.semaphore_signal(barrier, inc=1, device_id=peer, device_id_type=MESH)
    r = lax.broadcasted_iota(jnp.int32, (WINDOW, 2 * WINDOW), 0)
    k_ = lax.broadcasted_iota(jnp.int32, (WINDOW, 2 * WINDOW), 1)
    dist = WINDOW + r - k_
    near = (dist >= 0) & (dist <= WINDOW)
    bias_a[1] = jnp.where(near, 0.0, NEG)
    bias_a[0] = jnp.where(near & ((k_ >= WINDOW) | (sp > 0)), 0.0, NEG)
    r = lax.broadcasted_iota(jnp.int32, (WINDOW, 5 * WINDOW), 0)
    k_ = lax.broadcasted_iota(jnp.int32, (WINDOW, 5 * WINDOW), 1)
    back = lax.shift_right_logical(k_, 7)
    kr = k_ & 127
    db = lax.shift_right_logical(r, 5) - lax.shift_right_logical(kr, 5)
    dist = rows * back + 16 * ((r & 31) - (kr & 31)) + 4 * db
    seen = (dist >= 0) & (back <= sp)
    in16 = seen & (db == 0) & (dist <= 16 * WINDOW)
    in4 = seen & (dist <= 4 * WINDOW)
    bias_b[...] = jnp.where(in16 & in4, LN2, jnp.where(in16 | in4, 0.0, NEG))

    for cp in loads(True):
        cp.wait()
    pl.semaphore_wait(barrier, len(peers))

    z_to = [{"z": at_z(1)}, {"z": at_z(-1)}]
    y_to = [{"y": at_y(1)}, {"y": at_y(-1)}]
    partner = {"c": 1 - c}
    last = NZ // 2

    def arrived_all(ref, sem):
        remote(ref, ref, out_sem.at[0], sem, z_to[0]).wait_recv()

    def left_all(ref, sem):
        remote(ref, ref, sem, xd, z_to[0]).wait_send()

    def z_ref(flow, src, way, s):
        if flow < 3:
            lo, n = (2 * flow, 2) if s < last else (2 * flow + way, 1)
            return wz.at[src * NY + y, :, pl.ds(lo * lanes, n * lanes)]
        cols = pl.ds(src * NY, NY) if s < last else pl.ds(src * NY + 2 * way, 2)
        return wog.at[flow - 3, cols]

    def z_copy(flow, way, s, hop):
        ref = z_ref(flow, at_z(-hop if way == 0 else hop), way, s)
        return remote(ref, ref, out_sem.at[flow // 3], zr.at[flow, way, s - 1], z_to[way])

    def z_first(flow):
        for way in (0, 1):
            z_copy(flow, way, 1, 0).start()

    def z_hop(flow, s):
        for way in (0, 1):
            z_copy(flow, way, s, s).wait_recv()
            if s < last:
                z_copy(flow, way, s + 1, s).start()

    def y_copy(kind, slot, col):
        ref = wz.at[at_z(-slot) * NY + at_y(col)]
        split = 3 * lanes
        if kind == 2:
            ref = ref.at[:, pl.ds(0, split)]
        if kind == 3:
            ref = ref.at[:, pl.ds(split, 3 * lanes)]
        to = {"y": at_y(2)} if kind == 4 else y_to[kind % 2]
        return remote(
            ref, ref, out_sem.at[3 if kind < 2 else 2], yr.at[kind, slot] if kind < 2 else yd.at[slot], to
        )

    def y_send(slot):
        y_copy(0, slot, 0).start()
        y_copy(1, slot, 0).start()
        if slot in DIRECT:
            y_copy(4, slot, 0).start()

    def y_relay(slot):
        y_copy(0, slot, -1).wait_recv()
        if slot not in DIRECT:
            y_copy(2, slot, -1).start()
        y_copy(1, slot, 1).wait_recv()
        if slot not in DIRECT:
            y_copy(3, slot, 1).start()

    def y_done(slot):
        y_copy(4, slot, 2).wait_recv()
        row = pl.ds(at_z(-slot) * NY, NY)
        near = min(slot, NZ - slot)
        group = 0 if near <= 4 else 1 if near <= 6 else 2
        remote(wz.at[row, :, other], wz.at[row, :, mine], out_sem.at[4], push_r.at[group], partner).start()

    def o_push(slot):
        row = pl.ds(at_z(-slot) * NY, NY)
        group = X_ORDER.index(slot) // 4
        remote(wog.at[1, row], wog.at[0, row], out_sem.at[5], o_r.at[group], partner).start()

    def arrived(s):
        if s == 0:
            return [0]
        return [s, NZ - s] if s < last else [s]

    def x_copy(kind, slot):
        span = pl.ds(at_z(-slot) * NY, NY)
        way = (0, 1, slot % 2)[kind]
        src = wox.at[(2, 0)[way], span] if kind == 2 else wog.at[0, span]
        dst = wox.at[(2, 0, 1)[kind], span]
        return remote(
            src, dst, out_sem.at[7], xr.at[kind, X_ORDER.index(slot) // 8] if kind < 2 else xd,
            {"x": at_x(1 if way == 0 else -1)},
        )

    def x_send(slot):
        x_copy(0, slot).start()
        x_copy(1, slot).start()

    def x_relay(group):
        for kind in (0, 1):
            arrived_all(wox.at[0, pl.ds(0, 8 * NY)], xr.at[kind, group])
        for slot in X_ORDER[8 * group:8 * group + 8]:
            x_copy(2, slot).start()

    def row_send(item, d):
        ref = wog.at[item, sp]
        return remote(ref, ref, out_sem.at[8], row_r.at[item], {"y": at_y(d)})

    first = z - 4 + lax.rem(z, 2)

    def project(k):
        src = lax.rem(first + 2 * k + NZ, NZ)
        at = pl.multiple_of(src * (NY * shard), 2 * NY * shard)
        w = wz[pl.ds(src * NY, 2 * NY), :, 3 * lanes:].reshape(2 * NY * shard, 3 * lanes)
        return jnp.dot(tok[:, pl.ds(at, 2 * NY * shard)], w, preferred_element_type=F32)

    @pl.when(c == 0)
    def _():
        remote(wz.at[sp, :, other], wz.at[sp, :, other], out_sem.at[0], push_r.at[0], partner).start()
        remote(wog.at[1, sp], wog.at[1, sp], out_sem.at[1], push_r.at[1], partner).start()
        copy_tokens.wait()
        for group in range(4):
            arrived_all(wog.at[0, pl.ds(0, 4 * NY)], o_r.at[group])
            for slot in X_ORDER[4 * group:4 * group + 4]:
                x_send(slot)
            if group == 2:
                arrived_all(wz.at[pl.ds(0, 9 * NY), :, mine], push_r.at[0])
                acc[...] = project(0) + project(1) + project(2) + project(3)
        arrived_all(wz.at[pl.ds(0, 4 * NY), :, mine], push_r.at[1])
        acc[...] += project(-1) + project(4)
        arrived_all(wz.at[pl.ds(0, 3 * NY), :, mine], push_r.at[2])

    @pl.when(c == 1)
    def _():
        z_first(2)
        copy_tokens.wait()
        for d in (1, 3, 2):
            row_send(0, d).start()
        arrived_all(wz.at[sp, :, other], push_r.at[0])
        z_first(0)
        z_first(1)
        y_send(0)
        arrived_all(wog.at[1, sp], push_r.at[1])
        for d in (1, 3, 2):
            row_send(1, d).start()
        for s in range(1, last + O_LAG + 1):
            if s <= last:
                for flow in Z_FLOWS:
                    z_hop(flow, s)
                for slot in arrived(s):
                    y_send(slot)
            for item in (0, 1):
                if s == 1:
                    arrived_all(wog.at[0, pl.ds(0, NY - 1)], row_r.at[item])
                    z_first(3 + item)
                elif s > O_LAG:
                    z_hop(3 + item, s - O_LAG)
            for slot in [0] if s == 1 else arrived(s - O_LAG) if s > O_LAG else []:
                x_send(slot)
                o_push(slot)
            if Y_LAG <= s <= last + Y_LAG:
                for slot in arrived(s - Y_LAG):
                    y_relay(slot)
            if Y_DONE <= s <= last + Y_DONE:
                for slot in arrived(s - Y_DONE):
                    y_done(slot)
            if s == 4 + Y_DONE:
                acc[...] = project(0) + project(1) + project(2) + project(3)
            if s == 6 + Y_DONE:
                acc[...] += project(-1) + project(4)
        for s in range(last + O_LAG + 1, last + Y_DONE + 1):
            if s <= last + Y_LAG:
                for slot in arrived(s - Y_LAG):
                    y_relay(slot)
            for slot in arrived(s - Y_DONE):
                y_done(slot)

    x_relay(0)
    qkv = acc[...] + project(5) + project(6)
    for j in range(2):
        side = slice(j * lanes, (j + 1) * lanes)
        kvf[j, WINDOW:, :] = qkv[:, side]
        for e in range(4):
            for b in range(4):
                picked = kvf[j, pl.ds(WINDOW + 4 * b + e, 32, stride=16), :]
                halo[e, 0, 32 * b:32 * b + 32, side] = picked.astype(BF16)

    def prev_copy(e):
        return remote(halo.at[e, 0], halo.at[e, 4], out_sem.at[9], hr.at[0, e], z_to[0])

    def row_copy(e, k, src):
        return remote(halo.at[e, src], halo.at[e, k], out_sem.at[9], hr.at[k, e], {"y": at_y(k)})

    def relay_copy(e, k):
        return remote(halo.at[e, k], halo.at[e, 2], out_sem.at[12], hr.at[2, e], y_to[0 if k == 1 else 1])

    for e in range(4):
        prev_copy(e).start()
        for k in (1, 3):
            @pl.when((y + k < NY) & ((c == 0) | (e < 2)))
            def _():
                row_copy(e, k, 0).start()

    def wrap(e):
        prev_copy(e).wait_recv()
        for k in (1, 3):
            @pl.when(y + k >= NY)
            def _():
                row_copy(e, k, 4).start()

    def pass_on(e):
        row_copy(e, 1, 0).wait_recv()

        @pl.when((y == 2) | ((y < 2) & (e < 2)))
        def _():
            relay_copy(e, 1).start()

        row_copy(e, 3, 0).wait_recv()

        @pl.when((y == 1) | ((y >= 2) & (e >= 2)))
        def _():
            relay_copy(e, 3).start()

    qf[...] = qkv[:, 2 * lanes:].astype(BF16).astype(F32) * (HEAD ** -0.5)
    head0 = lax.broadcasted_iota(jnp.int32, (WINDOW, lanes), 1) < HEAD

    def attend(qb, kb, vb, bias):
        q0 = jnp.where(head0, qb, 0.0).astype(BF16)
        q1 = jnp.where(head0, 0.0, qb).astype(BF16)
        s = nt_dot(jnp.concatenate([q0, q1], 0), kb)
        probs, tops, sums = [], [], []
        for h in range(2):
            sh = s[h * WINDOW:(h + 1) * WINDOW] + bias
            top = jnp.max(sh, axis=1, keepdims=True)
            w = jnp.exp(sh - top)
            tops.append(top)
            sums.append(jnp.sum(w, axis=1, keepdims=True))
            probs.append(w.astype(BF16))
        o = jnp.dot(jnp.concatenate(probs, 0), vb, preferred_element_type=F32)
        out = jnp.where(head0, o[0:WINDOW], o[WINDOW:])
        return out, jnp.where(head0, tops[0], tops[1]), jnp.where(head0, sums[0], sums[1])

    def near_block(i):
        span = slice(i * WINDOW, (i + 1) * WINDOW)
        keys = slice(i * WINDOW, (i + 2) * WINDOW)
        out, top, total = attend(
            qf[span, :], kvf[0, keys, :].astype(BF16), kvf[1, keys, :].astype(BF16), bias_a[min(i, 1)]
        )
        oa[span, :] = out
        ma[span, :] = top
        la[span, :] = total

    for e in range(4):
        wrap(e)
        if e < 2:
            for k in (1, 3):
                @pl.when((y + k < NY) & (c == 1))
                def _():
                    row_copy(e + 2, k, 0).start()
        if e < 3:
            near_block(e + 1)
    x_relay(1)
    for e in range(4):
        pass_on(e)

    for e in range(4):
        for b in range(4):
            for j in range(2):
                tail = halo[e, 1, 32 * b + 24:32 * b + 32, j * lanes:(j + 1) * lanes]
                kvf[j, pl.ds(4 * b + e, 8, stride=16), :] = tail.astype(F32)
    near_block(0)

    for e in range(4):
        row_copy(e, 2, 0).wait_recv()
        pick = [pl.ds(4 * b + e, 32, stride=16) for b in range(4)]
        qb = jnp.concatenate([qf[p, :] for p in pick], 0)
        kvb = halo[e].reshape(5 * WINDOW, 2 * lanes)
        out, top, total = attend(qb, kvb[:, 0:lanes], kvb[:, lanes:], bias_b[...])
        o_a = jnp.concatenate([oa[p, :] for p in pick], 0)
        m_a = jnp.concatenate([ma[p, :] for p in pick], 0)
        l_a = jnp.concatenate([la[p, :] for p in pick], 0)
        peak = jnp.maximum(top, m_a)
        f_b = jnp.exp(top - peak)
        f_a = jnp.exp(m_a - peak)
        denom = f_a * l_a + f_b * total
        res = (f_a * o_a + f_b * out) / denom
        lse = peak + jnp.log(denom)
        for b in range(4):
            att[pick[b], :] = res[32 * b:32 * b + 32]
            lse_rows[pick[b], :] = lse[32 * b:32 * b + 32]

    att_b[...] = att[...].reshape(NX, rows // NX, lanes).astype(BF16)

    def att_copy(d):
        return remote(att_b.at[at_x(d)], att_x.at[NX - d], out_sem.at[10], ar.at[d - 1], {"x": at_x(d)})

    for d in (1, 3, 2):
        att_copy(d).start()
    att_x[0] = att_b[x]
    lse_t = lse_rows[...].T
    lse_out[0:1, :] = lse_t[0:1, :]
    lse_out[1:2, :] = lse_t[HEAD:HEAD + 1, :]
    groups = 8
    width = NZ * NY // groups
    hrows = rows // NX // 2
    for g in range(groups):
        w_own = wog[0, g * width:(g + 1) * width].reshape(width * shard, lanes)
        part[g] = nt_dot(att_x[0], w_own).reshape(2, hrows, width * shard)
    for d in (1, 3):
        att_copy(NX - d).wait_recv()
        for g in range(groups):
            w_k = wox[d - 1, g * width:(g + 1) * width].reshape(width * shard, lanes)
            part[g] += nt_dot(att_x[d], w_k).reshape(2, hrows, width * shard)
    arrived_all(wox.at[1], xd)
    att_copy(2).wait_recv()

    def core_copy(j):
        at = pl.ds(j * groups // 2, groups // 2)
        return remote(part_b.at[at, 1 - c], theirs.at[at], out_sem.at[11], cr, {"c": 1 - c})

    for g in range(groups):
        span = slice(g * width, (g + 1) * width)
        acc = nt_dot(att_x[2], wox[1, span].reshape(width * shard, lanes))
        part_b[g] = (acc.reshape(2, hrows, width * shard) + part[g]).astype(BF16)
        if g % (groups // 2) == groups // 2 - 1:
            core_copy(g * 2 // groups).start()
    pltpu.make_async_copy(part_b.at[:, c], ours, load_sem.at[1]).start()
    remote(part_b.at[:, c], theirs, out_sem.at[11], cr, partner).wait_recv()
    pltpu.make_async_copy(part_b.at[:, c], ours, load_sem.at[1]).wait()
    @pl.when(c == 0)
    def _():
        left_all(wz.at[sp, :, other], out_sem.at[0])
        left_all(wog.at[1, sp], out_sem.at[1])

    @pl.when(c == 1)
    def _():
        left_all(wz.at[pl.ds(0, NZ - 1)], out_sem.at[0])
        left_all(wog.at[:, pl.ds(0, (NZ - 1) * NY)], out_sem.at[1])
        left_all(wz.at[pl.ds(0, 2 * NZ)], out_sem.at[3])
        left_all(wz.at[pl.ds(0, NZ)], out_sem.at[2])
        left_all(wz.at[:, :, mine], out_sem.at[4])
        left_all(wog.at[0], out_sem.at[5])
        left_all(wog.at[:, pl.ds(0, NY - 1)], out_sem.at[8])

    left_all(wox, out_sem.at[7])
    left_all(halo.at[:, pl.ds(0, 3)], out_sem.at[9])
    left_all(halo.at[0, pl.ds(0, 2)], out_sem.at[12])

    @pl.when((y == 1) | (y == 2))
    def _():
        left_all(halo.at[:, 0], out_sem.at[12])

    left_all(att_x.at[pl.ds(1, NX - 1)], out_sem.at[10])
    left_all(part_b.at[:, c], out_sem.at[11])


def sum_kernel(ours, theirs, lse, mixed, lse_out):
    wide = ours.shape[2]
    for g in range(ours.shape[0]):
        total = ours[g].astype(F32) + theirs[g].astype(F32)
        mixed[:, g * wide:(g + 1) * wide] = total.astype(BF16)
    lse_out[...] = lse[...]


def shards(tokens, w_query, w_key, w_value, w_out):
    rows, depth = tokens.shape
    shard, lanes = w_query.shape
    n_sp = NZ * NY
    groups = 8
    wide = n_sp // groups * shard
    vmem = pl.BlockSpec(memory_space=pltpu.VMEM)
    anywhere = pl.BlockSpec(memory_space=pl.ANY)
    dma = pltpu.SemaphoreType.DMA
    ours, theirs, lse = pl.pallas_call(
        layer_kernel,
        name="layer",
        out_shape=(
            jax.ShapeDtypeStruct((groups, rows // 8, wide), BF16),
            jax.ShapeDtypeStruct((groups, rows // 8, wide), BF16),
            jax.ShapeDtypeStruct((2, rows), F32),
        ),
        in_specs=[pl.BlockSpec(memory_space=pl.ANY)] * 5,
        out_specs=(anywhere, anywhere, vmem),
        scratch_shapes=[
            pltpu.VMEM((rows, depth), BF16),
            pltpu.VMEM((rows, 3 * lanes), F32),
            pltpu.VMEM((n_sp, shard, 6 * lanes), BF16),
            pltpu.VMEM((2, n_sp, shard, lanes), BF16),
            pltpu.VMEM((NX - 1, n_sp, shard, lanes), BF16),
            pltpu.VMEM((4, 5, WINDOW, 2 * lanes), BF16),
            pltpu.VMEM((rows, lanes), F32),
            pltpu.VMEM((2, WINDOW + rows, lanes), F32),
            pltpu.VMEM((rows, lanes), F32),
            pltpu.VMEM((rows, lanes), F32),
            pltpu.VMEM((rows, lanes), F32),
            pltpu.VMEM((rows, lanes), F32),
            pltpu.VMEM((rows, lanes), F32),
            pltpu.VMEM((NX, rows // NX, lanes), BF16),
            pltpu.VMEM((NX, rows // NX, lanes), BF16),
            pltpu.VMEM((groups, 2, rows // NX // 2, wide), F32),
            pltpu.VMEM((groups, 2, rows // NX // 2, wide), BF16),
            pltpu.VMEM((2, WINDOW, 2 * WINDOW), F32),
            pltpu.VMEM((WINDOW, 5 * WINDOW), F32),
            dma((5,)),
            dma((13,)),
            dma((2,)),
            dma((5, 2, NZ // 2)),
            dma((2, NZ)),
            dma((NZ,)),
            dma((3,)),
            dma((4,)),
            dma((2, 2)),
            dma,
            dma((4, 4)),
            dma((3,)),
            dma,
        ],
        compiler_params=pltpu.CompilerParams(
            collective_id=0, has_side_effects=True, vmem_limit_bytes=60 * 1024 * 1024
        ),
    )(tokens, w_query, w_key, w_value, w_out.T)
    return pl.pallas_call(
        sum_kernel,
        name="total",
        out_shape=(
            jax.ShapeDtypeStruct((rows // 8, depth), BF16),
            jax.ShapeDtypeStruct((2, rows), F32),
        ),
        in_specs=[vmem] * 3,
        out_specs=(vmem, vmem),
    )(ours, theirs, lse)


def solution(mesh):
    torus = Mesh(mesh.devices.reshape(NZ, NY, NX, 2), ("z", "y", "x", "c"))
    in_specs = (P(SP, None), P(SP, TP), P(SP, TP), P(SP, TP), P(TP, SP))
    out_specs = (P(SP + TP, None), P(TP, SP))
    return jax.shard_map(
        shards, mesh=torus, in_specs=in_specs, out_specs=out_specs, check_vma=False
    )
```

```python
import jax
import jax.numpy as jnp
from jax import lax
from jax.experimental import pallas as pl
from jax.experimental.pallas import tpu as pltpu
from jax.sharding import Mesh
from jax.sharding import PartitionSpec as P

HEAD = 64
WINDOW = 128
NZ = 16
NY = 4
NX = 4
MESH = pl.DeviceIdType.MESH
SP = ("z", "y")
TP = ("x", "c")
NEG = -1e30
LN2 = 0.6931471805599453
F32 = jnp.float32
BF16 = jnp.bfloat16
X_ORDER = [0] + [v for s in range(1, NZ // 2) for v in (s, NZ - s)] + [NZ // 2]


O_LAG = 1
Y_LAG = 1
Y_DONE = 3
Z_FLOWS = (2, 1, 0)
DIRECT = (NZ // 2,)


def nt_dot(a, b):
    return lax.dot_general(a, b, (((1,), (1,)), ((), ())), preferred_element_type=F32)


def remote(src, dst, send, recv, device):
    return pltpu.make_async_remote_copy(
        src_ref=src, dst_ref=dst, send_sem=send, recv_sem=recv, device_id=device, device_id_type=MESH
    )


def layer_kernel(
    tokens, wq, wk_in, wv, wo, ours, theirs, lse_out,
    tok, acc, wz, wog, wox, halo, qf, kvf, oa, ma, la, att, lse_rows, lse_v, att_b, att_x, part, part_b,
    bias_a, bias_b,
    load_sem, out_sem, row_r, zr, yr, yd, push_r, o_r, xr, xd, hr, ar, cr,
):
    z, y, x, c = (lax.axis_index(n) for n in ("z", "y", "x", "c"))
    sp = z * NY + y
    shard, lanes = wk_in.shape
    rows = tokens.shape[0]
    other = pl.ds(0, 3 * lanes)
    mine = pl.ds(3 * lanes, 3 * lanes)

    def load(src, dst, k):
        return pltpu.make_async_copy(src, dst, load_sem.at[k])

    def loads(first):
        lo, slot = (0, 1) if first else (3 * lanes, 0)
        return [
            load(wk_in, wz.at[sp, :, pl.ds(lo, lanes)], 1),
            load(wv, wz.at[sp, :, pl.ds(lo + lanes, lanes)], 2),
            load(wq, wz.at[sp, :, pl.ds(lo + 2 * lanes, lanes)], 3),
            load(wo, wog.at[slot, sp], 4),
        ]

    for core in (0, 1):
        @pl.when(c == core)
        def _():
            for cp in loads(core == 0):
                cp.start()
    copy_tokens = load(tokens, tok, 0)
    copy_tokens.start()

    def at_z(d):
        return lax.rem(z + d + NZ, NZ)

    def at_y(d):
        return lax.rem(y + d + NY, NY)

    def at_x(d):
        return lax.rem(x + d + NX, NX)

    barrier = pltpu.get_barrier_semaphore()
    peers = [{"z": at_z(1)}, {"z": at_z(-1)}]
    peers += [{"y": at_y(d)} for d in range(1, NY)]
    peers += [{"x": at_x(d)} for d in range(1, NX)]
    peers += [{"c": 1 - c}]
    peers += [{"z": at_z(d), "c": 1 - c} for d in (1, -1)] + [{"y": at_y(d), "c": 1 - c} for d in range(1, NY)]
    for peer in peers:
        pl.semaphore_signal(barrier, inc=1, device_id=peer, device_id_type=MESH)
    r = lax.broadcasted_iota(jnp.int32, (WINDOW, 2 * WINDOW), 0)
    k_ = lax.broadcasted_iota(jnp.int32, (WINDOW, 2 * WINDOW), 1)
    dist = WINDOW + r - k_
    near = (dist >= 0) & (dist <= WINDOW)
    bias_a[1] = jnp.where(near, 0.0, NEG)
    bias_a[0] = jnp.where(near & ((k_ >= WINDOW) | (sp > 0)), 0.0, NEG)
    r = lax.broadcasted_iota(jnp.int32, (WINDOW, 5 * WINDOW), 0)
    k_ = lax.broadcasted_iota(jnp.int32, (WINDOW, 5 * WINDOW), 1)
    back = lax.shift_right_logical(k_, 7)
    kr = k_ & 127
    db = lax.shift_right_logical(r, 5) - lax.shift_right_logical(kr, 5)
    dist = rows * back + 16 * ((r & 31) - (kr & 31)) + 4 * db
    seen = (dist >= 0) & (back <= sp)
    in16 = seen & (db == 0) & (dist <= 16 * WINDOW)
    in4 = seen & (dist <= 4 * WINDOW)
    bias_b[...] = jnp.where(in16 & in4, LN2, jnp.where(in16 | in4, 0.0, NEG))

    for cp in loads(True):
        cp.wait()
    pl.semaphore_wait(barrier, len(peers))

    z_to = [{"z": at_z(1)}, {"z": at_z(-1)}]
    y_to = [{"y": at_y(1)}, {"y": at_y(-1)}]
    partner = {"c": 1 - c}
    last = NZ // 2

    def arrived_all(ref, sem):
        remote(ref, ref, out_sem.at[0], sem, z_to[0]).wait_recv()

    def left_all(ref, sem):
        remote(ref, ref, sem, xd, z_to[0]).wait_send()

    def z_ref(flow, src, way, s):
        if flow < 3:
            lo, n = (2 * flow, 2) if s < last else (2 * flow + way, 1)
            return wz.at[src * NY + y, :, pl.ds(lo * lanes, n * lanes)]
        cols = pl.ds(src * NY, NY) if s < last else pl.ds(src * NY + 2 * way, 2)
        return wog.at[flow - 3, cols]

    def z_copy(flow, way, s, hop):
        ref = z_ref(flow, at_z(-hop if way == 0 else hop), way, s)
        return remote(ref, ref, out_sem.at[flow // 3], zr.at[flow, way, s - 1], z_to[way])

    def z_first(flow):
        for way in (0, 1):
            z_copy(flow, way, 1, 0).start()

    def z_hop(flow, s):
        for way in (0, 1):
            z_copy(flow, way, s, s).wait_recv()
            if s < last:
                z_copy(flow, way, s + 1, s).start()

    def y_copy(kind, slot, col):
        ref = wz.at[at_z(-slot) * NY + at_y(col)]
        split = 3 * lanes
        if kind == 2:
            ref = ref.at[:, pl.ds(0, split)]
        if kind == 3:
            ref = ref.at[:, pl.ds(split, 3 * lanes)]
        to = {"y": at_y(2)} if kind == 4 else y_to[kind % 2]
        return remote(
            ref, ref, out_sem.at[3 if kind < 2 else 2], yr.at[kind, slot] if kind < 2 else yd.at[slot], to
        )

    def y_send(slot):
        y_copy(0, slot, 0).start()
        y_copy(1, slot, 0).start()
        if slot in DIRECT:
            y_copy(4, slot, 0).start()

    def y_relay(slot):
        y_copy(0, slot, -1).wait_recv()
        if slot not in DIRECT:
            y_copy(2, slot, -1).start()
        y_copy(1, slot, 1).wait_recv()
        if slot not in DIRECT:
            y_copy(3, slot, 1).start()

    def y_done(slot):
        y_copy(4, slot, 2).wait_recv()
        row = pl.ds(at_z(-slot) * NY, NY)
        near = min(slot, NZ - slot)
        group = 0 if near <= 4 else 1 if near <= 6 else 2
        remote(wz.at[row, :, other], wz.at[row, :, mine], out_sem.at[4], push_r.at[group], partner).start()

    def o_push(slot):
        row = pl.ds(at_z(-slot) * NY, NY)
        group = X_ORDER.index(slot) // 4
        remote(wog.at[1, row], wog.at[0, row], out_sem.at[5], o_r.at[group], partner).start()

    def arrived(s):
        if s == 0:
            return [0]
        return [s, NZ - s] if s < last else [s]

    def x_copy(kind, slot):
        span = pl.ds(at_z(-slot) * NY, NY)
        way = (0, 1, slot % 2)[kind]
        src = wox.at[(2, 0)[way], span] if kind == 2 else wog.at[0, span]
        dst = wox.at[(2, 0, 1)[kind], span]
        return remote(
            src, dst, out_sem.at[7], xr.at[kind, X_ORDER.index(slot) // 8] if kind < 2 else xd,
            {"x": at_x(1 if way == 0 else -1)},
        )

    def x_send(slot):
        x_copy(0, slot).start()
        x_copy(1, slot).start()

    def x_relay(group):
        for kind in (0, 1):
            arrived_all(wox.at[0, pl.ds(0, 8 * NY)], xr.at[kind, group])
        for slot in X_ORDER[8 * group:8 * group + 8]:
            x_copy(2, slot).start()

    def row_send(item, d):
        ref = wog.at[item, sp]
        return remote(ref, ref, out_sem.at[8], row_r.at[item], {"y": at_y(d)})

    first = z - 4 + lax.rem(z, 2)

    def project(k):
        src = lax.rem(first + 2 * k + NZ, NZ)
        at = pl.multiple_of(src * (NY * shard), 2 * NY * shard)
        w = wz[pl.ds(src * NY, 2 * NY), :, 3 * lanes:].reshape(2 * NY * shard, 3 * lanes)
        return jnp.dot(tok[:, pl.ds(at, 2 * NY * shard)], w, preferred_element_type=F32)

    def first_sends(ref):
        for way in (0, 1):
            remote(ref, ref, out_sem.at[0], zr.at[0, way, 0], {"z": at_z(1 - 2 * way), "c": 1}).start()
        for kind in (0, 1):
            remote(ref, ref, out_sem.at[0], yr.at[kind, 0], {"y": at_y(1 - 2 * kind), "c": 1}).start()

    @pl.when(c == 0)
    def _():
        first_sends(wz.at[sp, :, other])
        for d in (1, 3, 2):
            at = {"y": at_y(d), "c": 1}
            remote(wog.at[1, sp], wog.at[1, sp], out_sem.at[1], row_r.at[1], at).start()
        remote(wog.at[1, sp], wog.at[1, sp], out_sem.at[1], push_r.at[1], partner).start()
        remote(wz.at[sp, :, other], wz.at[sp, :, other], out_sem.at[0], push_r.at[0], partner).start()
        copy_tokens.wait()
        for group in range(4):
            arrived_all(wog.at[0, pl.ds(0, 4 * NY)], o_r.at[group])
            for slot in X_ORDER[4 * group:4 * group + 4]:
                x_send(slot)
            if group == 2:
                arrived_all(wz.at[pl.ds(0, 9 * NY), :, mine], push_r.at[0])
                acc[...] = project(0) + project(1) + project(2) + project(3)
        arrived_all(wz.at[pl.ds(0, 4 * NY), :, mine], push_r.at[1])
        acc[...] += project(-1) + project(4)
        arrived_all(wz.at[pl.ds(0, 3 * NY), :, mine], push_r.at[2])

    @pl.when(c == 1)
    def _():
        first_sends(wz.at[sp, :, mine])
        for d in (1, 3, 2):
            row_send(0, d).start()
        copy_tokens.wait()
        arrived_all(wog.at[1, sp], push_r.at[1])
        arrived_all(wz.at[sp, :, other], push_r.at[0])
        for s in range(1, last + O_LAG + 1):
            if s <= last:
                if s == 1:
                    for way in (0, 1):
                        arrived_all(wz.at[sp], zr.at[0, way, 0])
                        for flow in Z_FLOWS:
                            z_copy(flow, way, 2, 1).start()
                else:
                    for flow in Z_FLOWS:
                        z_hop(flow, s)
                for slot in arrived(s):
                    y_send(slot)
            for item in (0, 1):
                if s == 1:
                    arrived_all(wog.at[0, pl.ds(0, NY - 1)], row_r.at[item])
                    z_first(3 + item)
                elif s > O_LAG:
                    z_hop(3 + item, s - O_LAG)
            for slot in [0] if s == 1 else arrived(s - O_LAG) if s > O_LAG else []:
                x_send(slot)
                o_push(slot)
            if Y_LAG <= s <= last + Y_LAG:
                for slot in arrived(s - Y_LAG):
                    y_relay(slot)
            if Y_DONE <= s <= last + Y_DONE:
                for slot in arrived(s - Y_DONE):
                    y_done(slot)
            if s == 4 + Y_DONE:
                acc[...] = project(0) + project(1) + project(2) + project(3)
            if s == 6 + Y_DONE:
                acc[...] += project(-1) + project(4)
        for s in range(last + O_LAG + 1, last + Y_DONE + 1):
            if s <= last + Y_LAG:
                for slot in arrived(s - Y_LAG):
                    y_relay(slot)
            for slot in arrived(s - Y_DONE):
                y_done(slot)

    x_relay(0)
    qkv = acc[...] + project(5) + project(6)
    for j in range(2):
        side = slice(j * lanes, (j + 1) * lanes)
        kvf[j, WINDOW:, :] = qkv[:, side]
        for e in range(4):
            for b in range(4):
                picked = kvf[j, pl.ds(WINDOW + 4 * b + e, 32, stride=16), :]
                halo[e, 0, 32 * b:32 * b + 32, side] = picked.astype(BF16)

    def prev_copy(e):
        return remote(halo.at[e, 0], halo.at[e, 4], out_sem.at[9], hr.at[0, e], z_to[0])

    def row_copy(e, k, src):
        return remote(halo.at[e, src], halo.at[e, k], out_sem.at[9], hr.at[k, e], {"y": at_y(k)})

    def relay_copy(e, k):
        return remote(halo.at[e, k], halo.at[e, 2], out_sem.at[12], hr.at[2, e], y_to[0 if k == 1 else 1])

    for e in range(4):
        prev_copy(e).start()
        for k in (1, 3):
            @pl.when((y + k < NY) & ((c == 0) | (e < 2)))
            def _():
                row_copy(e, k, 0).start()

    def wrap(e):
        prev_copy(e).wait_recv()
        for k in (1, 3):
            @pl.when(y + k >= NY)
            def _():
                row_copy(e, k, 4).start()

    def pass_on(e):
        row_copy(e, 1, 0).wait_recv()

        @pl.when((y == 2) | ((y < 2) & (e < 2)))
        def _():
            relay_copy(e, 1).start()

        row_copy(e, 3, 0).wait_recv()

        @pl.when((y == 1) | ((y >= 2) & (e >= 2)))
        def _():
            relay_copy(e, 3).start()

    qf[...] = qkv[:, 2 * lanes:].astype(BF16).astype(F32) * (HEAD ** -0.5)
    head0 = lax.broadcasted_iota(jnp.int32, (WINDOW, lanes), 1) < HEAD

    def attend(qb, kb, vb, bias):
        q0 = jnp.where(head0, qb, 0.0).astype(BF16)
        q1 = jnp.where(head0, 0.0, qb).astype(BF16)
        s = nt_dot(jnp.concatenate([q0, q1], 0), kb)
        probs, tops, sums = [], [], []
        for h in range(2):
            sh = s[h * WINDOW:(h + 1) * WINDOW] + bias
            top = jnp.max(sh, axis=1, keepdims=True)
            w = jnp.exp(sh - top)
            tops.append(top)
            sums.append(jnp.sum(w, axis=1, keepdims=True))
            probs.append(w.astype(BF16))
        o = jnp.dot(jnp.concatenate(probs, 0), vb, preferred_element_type=F32)
        out = jnp.where(head0, o[0:WINDOW], o[WINDOW:])
        return out, jnp.where(head0, tops[0], tops[1]), jnp.where(head0, sums[0], sums[1])

    def near_block(i):
        span = slice(i * WINDOW, (i + 1) * WINDOW)
        keys = slice(i * WINDOW, (i + 2) * WINDOW)
        out, top, total = attend(
            qf[span, :], kvf[0, keys, :].astype(BF16), kvf[1, keys, :].astype(BF16), bias_a[min(i, 1)]
        )
        oa[span, :] = out
        ma[span, :] = top
        la[span, :] = total

    for e in range(4):
        wrap(e)
        if e < 2:
            for k in (1, 3):
                @pl.when((y + k < NY) & (c == 1))
                def _():
                    row_copy(e + 2, k, 0).start()
        if e < 3:
            near_block(e + 1)
    x_relay(1)
    for e in range(4):
        pass_on(e)

    for e in range(4):
        for b in range(4):
            for j in range(2):
                tail = halo[e, 1, 32 * b + 24:32 * b + 32, j * lanes:(j + 1) * lanes]
                kvf[j, pl.ds(4 * b + e, 8, stride=16), :] = tail.astype(F32)
    near_block(0)

    for e in range(4):
        row_copy(e, 2, 0).wait_recv()
        pick = [pl.ds(4 * b + e, 32, stride=16) for b in range(4)]
        qb = jnp.concatenate([qf[p, :] for p in pick], 0)
        kvb = halo[e].reshape(5 * WINDOW, 2 * lanes)
        out, top, total = attend(qb, kvb[:, 0:lanes], kvb[:, lanes:], bias_b[...])
        o_a = jnp.concatenate([oa[p, :] for p in pick], 0)
        m_a = jnp.concatenate([ma[p, :] for p in pick], 0)
        l_a = jnp.concatenate([la[p, :] for p in pick], 0)
        peak = jnp.maximum(top, m_a)
        f_b = jnp.exp(top - peak)
        f_a = jnp.exp(m_a - peak)
        denom = f_a * l_a + f_b * total
        res = (f_a * o_a + f_b * out) / denom
        lse = peak + jnp.log(denom)
        for b in range(4):
            att[pick[b], :] = res[32 * b:32 * b + 32]
            lse_rows[pick[b], :] = lse[32 * b:32 * b + 32]

    att_b[...] = att[...].reshape(NX, rows // NX, lanes).astype(BF16)

    def att_copy(d):
        return remote(att_b.at[at_x(d)], att_x.at[NX - d], out_sem.at[10], ar.at[d - 1], {"x": at_x(d)})

    for d in (1, 3, 2):
        att_copy(d).start()
    att_x[0] = att_b[x]
    lse_t = lse_rows[...].T
    lse_v[0:1, :] = lse_t[0:1, :]
    lse_v[1:2, :] = lse_t[HEAD:HEAD + 1, :]
    copy_lse = pltpu.make_async_copy(lse_v, lse_out, load_sem.at[2])
    copy_lse.start()
    groups = 8
    width = NZ * NY // groups
    hrows = rows // NX // 2
    for g in range(groups):
        w_own = wog[0, g * width:(g + 1) * width].reshape(width * shard, lanes)
        part[g] = nt_dot(att_x[0], w_own).reshape(2, hrows, width * shard)
    for d in (1, 3):
        att_copy(NX - d).wait_recv()
        for g in range(groups):
            w_k = wox[d - 1, g * width:(g + 1) * width].reshape(width * shard, lanes)
            part[g] += nt_dot(att_x[d], w_k).reshape(2, hrows, width * shard)
    arrived_all(wox.at[1], xd)
    att_copy(2).wait_recv()

    def core_copy(j):
        at = pl.ds(j * groups // 2, groups // 2)
        return remote(part_b.at[at, 1 - c], theirs.at[at], out_sem.at[11], cr, {"c": 1 - c})

    for g in range(groups):
        span = slice(g * width, (g + 1) * width)
        acc = nt_dot(att_x[2], wox[1, span].reshape(width * shard, lanes))
        part_b[g] = (acc.reshape(2, hrows, width * shard) + part[g]).astype(BF16)
        if g % (groups // 2) == groups // 2 - 1:
            core_copy(g * 2 // groups).start()
    pltpu.make_async_copy(part_b.at[:, c], ours, load_sem.at[1]).start()
    remote(part_b.at[:, c], theirs, out_sem.at[11], cr, partner).wait_recv()
    pltpu.make_async_copy(part_b.at[:, c], ours, load_sem.at[1]).wait()
    copy_lse.wait()
    @pl.when(c == 0)
    def _():
        left_all(wz.at[pl.ds(0, 5), :, other], out_sem.at[0])
        left_all(wog.at[0, pl.ds(0, NY)], out_sem.at[1])

    @pl.when(c == 1)
    def _():
        left_all(wz.at[pl.ds(0, NZ - 1)], out_sem.at[0])
        left_all(wog.at[:, pl.ds(0, (NZ - 1) * NY)], out_sem.at[1])
        left_all(wz.at[pl.ds(0, 2 * NZ - 2)], out_sem.at[3])
        left_all(wz.at[pl.ds(0, NZ)], out_sem.at[2])
        left_all(wz.at[:, :, mine], out_sem.at[4])
        left_all(wog.at[0], out_sem.at[5])
        left_all(wog.at[0, pl.ds(0, NY - 1)], out_sem.at[8])

    left_all(wox, out_sem.at[7])
    left_all(halo.at[:, pl.ds(0, 3)], out_sem.at[9])
    left_all(halo.at[0, pl.ds(0, 2)], out_sem.at[12])

    @pl.when((y == 1) | (y == 2))
    def _():
        left_all(halo.at[:, 0], out_sem.at[12])

    left_all(att_x.at[pl.ds(1, NX - 1)], out_sem.at[10])
    left_all(part_b.at[:, c], out_sem.at[11])


def sum_kernel(ours, theirs, lse, mixed, lse_out):
    wide = ours.shape[2]
    for g in range(ours.shape[0]):
        total = ours[g].astype(F32) + theirs[g].astype(F32)
        mixed[:, g * wide:(g + 1) * wide] = total.astype(BF16)
    lse_out[...] = lse[...]


def shards(tokens, w_query, w_key, w_value, w_out):
    rows, depth = tokens.shape
    shard, lanes = w_query.shape
    n_sp = NZ * NY
    groups = 8
    wide = n_sp // groups * shard
    vmem = pl.BlockSpec(memory_space=pltpu.VMEM)
    anywhere = pl.BlockSpec(memory_space=pl.ANY)
    dma = pltpu.SemaphoreType.DMA
    ours, theirs, lse = pl.pallas_call(
        layer_kernel,
        name="layer",
        out_shape=(
            jax.ShapeDtypeStruct((groups, rows // 8, wide), BF16),
            jax.ShapeDtypeStruct((groups, rows // 8, wide), BF16),
            jax.ShapeDtypeStruct((2, rows), F32),
        ),
        in_specs=[pl.BlockSpec(memory_space=pl.ANY)] * 5,
        out_specs=(anywhere, anywhere, anywhere),
        scratch_shapes=[
            pltpu.VMEM((rows, depth), BF16),
            pltpu.VMEM((rows, 3 * lanes), F32),
            pltpu.VMEM((n_sp, shard, 6 * lanes), BF16),
            pltpu.VMEM((2, n_sp, shard, lanes), BF16),
            pltpu.VMEM((NX - 1, n_sp, shard, lanes), BF16),
            pltpu.VMEM((4, 5, WINDOW, 2 * lanes), BF16),
            pltpu.VMEM((rows, lanes), F32),
            pltpu.VMEM((2, WINDOW + rows, lanes), F32),
            pltpu.VMEM((rows, lanes), F32),
            pltpu.VMEM((rows, lanes), F32),
            pltpu.VMEM((rows, lanes), F32),
            pltpu.VMEM((rows, lanes), F32),
            pltpu.VMEM((rows, lanes), F32),
            pltpu.VMEM((2, rows), F32),
            pltpu.VMEM((NX, rows // NX, lanes), BF16),
            pltpu.VMEM((NX, rows // NX, lanes), BF16),
            pltpu.VMEM((groups, 2, rows // NX // 2, wide), F32),
            pltpu.VMEM((groups, 2, rows // NX // 2, wide), BF16),
            pltpu.VMEM((2, WINDOW, 2 * WINDOW), F32),
            pltpu.VMEM((WINDOW, 5 * WINDOW), F32),
            dma((5,)),
            dma((13,)),
            dma((2,)),
            dma((5, 2, NZ // 2)),
            dma((2, NZ)),
            dma((NZ,)),
            dma((3,)),
            dma((4,)),
            dma((2, 2)),
            dma,
            dma((4, 4)),
            dma((3,)),
            dma,
        ],
        compiler_params=pltpu.CompilerParams(
            collective_id=0, has_side_effects=True, vmem_limit_bytes=60 * 1024 * 1024
        ),
    )(tokens, w_query, w_key, w_value, w_out.T)
    return pl.pallas_call(
        sum_kernel,
        name="total",
        out_shape=(
            jax.ShapeDtypeStruct((rows // 8, depth), BF16),
            jax.ShapeDtypeStruct((2, rows), F32),
        ),
        in_specs=[vmem] * 3,
        out_specs=(vmem, vmem),
    )(ours, theirs, lse)


def solution(mesh):
    torus = Mesh(mesh.devices.reshape(NZ, NY, NX, 2), ("z", "y", "x", "c"))
    in_specs = (P(SP, None), P(SP, TP), P(SP, TP), P(SP, TP), P(TP, SP))
    out_specs = (P(SP + TP, None), P(TP, SP))
    return jax.shard_map(
        shards, mesh=torus, in_specs=in_specs, out_specs=out_specs, check_vma=False
    )
```

```python
import jax
import jax.numpy as jnp
from jax import lax
from jax.experimental import pallas as pl
from jax.experimental.pallas import tpu as pltpu
from jax.sharding import Mesh
from jax.sharding import PartitionSpec as P

HEAD = 64
WINDOW = 128
NZ = 16
NY = 4
NX = 4
MESH = pl.DeviceIdType.MESH
SP = ("z", "y")
TP = ("x", "c")
NEG = -1e30
LN2 = 0.6931471805599453
F32 = jnp.float32
BF16 = jnp.bfloat16
X_ORDER = [0] + [v for s in range(1, NZ // 2) for v in (s, NZ - s)] + [NZ // 2]


O_LAG = 1
Y_LAG = 1
Y_DONE = 3
Z_FLOWS = (2, 1, 0)
DIRECT = (NZ // 2,)


def nt_dot(a, b):
    return lax.dot_general(a, b, (((1,), (1,)), ((), ())), preferred_element_type=F32)


def remote(src, dst, send, recv, device):
    return pltpu.make_async_remote_copy(
        src_ref=src, dst_ref=dst, send_sem=send, recv_sem=recv, device_id=device, device_id_type=MESH
    )


def layer_kernel(
    tokens, wq, wk_in, wv, wo, ours, theirs, lse_out,
    tok, acc, wz, wog, woxs, woxm, halo, qf, kvf, oa, ma, la, att, lse_rows, lse_v, att_b, att_x, part, part_b,
    bias_a, bias_b,
    load_sem, out_sem, row_r, zr, yr, yd, push_r, o_r, xr, xd, hr, ar, cr,
):
    z, y, x, c = (lax.axis_index(n) for n in ("z", "y", "x", "c"))
    sp = z * NY + y
    shard, lanes = wk_in.shape
    rows = tokens.shape[0]
    other = pl.ds(0, 3 * lanes)
    mine = pl.ds(3 * lanes, 3 * lanes)

    def load(src, dst, k):
        return pltpu.make_async_copy(src, dst, load_sem.at[k])

    def loads(first):
        lo, slot = (0, 1) if first else (3 * lanes, 0)
        return [
            load(wk_in, wz.at[sp, :, pl.ds(lo, lanes)], 1),
            load(wv, wz.at[sp, :, pl.ds(lo + lanes, lanes)], 2),
            load(wq, wz.at[sp, :, pl.ds(lo + 2 * lanes, lanes)], 3),
            load(wo, wog.at[slot, sp], 4),
        ]

    for core in (0, 1):
        @pl.when(c == core)
        def _():
            for cp in loads(core == 0):
                cp.start()
    copy_tokens = load(tokens, tok, 0)
    copy_tokens.start()

    def at_z(d):
        return lax.rem(z + d + NZ, NZ)

    def at_y(d):
        return lax.rem(y + d + NY, NY)

    def at_x(d):
        return lax.rem(x + d + NX, NX)

    barrier = pltpu.get_barrier_semaphore()
    peers = [{"z": at_z(1)}, {"z": at_z(-1)}]
    peers += [{"y": at_y(d)} for d in range(1, NY)]
    peers += [{"x": at_x(d)} for d in range(1, NX)]
    peers += [{"c": 1 - c}]
    peers += [{"z": at_z(d), "c": 1 - c} for d in (1, -1)] + [{"y": at_y(d), "c": 1 - c} for d in range(1, NY)]
    for peer in peers:
        pl.semaphore_signal(barrier, inc=1, device_id=peer, device_id_type=MESH)
    r = lax.broadcasted_iota(jnp.int32, (WINDOW, 2 * WINDOW), 0)
    k_ = lax.broadcasted_iota(jnp.int32, (WINDOW, 2 * WINDOW), 1)
    dist = WINDOW + r - k_
    near = (dist >= 0) & (dist <= WINDOW)
    bias_a[1] = jnp.where(near, 0.0, NEG)
    bias_a[0] = jnp.where(near & ((k_ >= WINDOW) | (sp > 0)), 0.0, NEG)
    r = lax.broadcasted_iota(jnp.int32, (WINDOW, 5 * WINDOW), 0)
    k_ = lax.broadcasted_iota(jnp.int32, (WINDOW, 5 * WINDOW), 1)
    back = lax.shift_right_logical(k_, 7)
    kr = k_ & 127
    db = lax.shift_right_logical(r, 5) - lax.shift_right_logical(kr, 5)
    dist = rows * back + 16 * ((r & 31) - (kr & 31)) + 4 * db
    seen = (dist >= 0) & (back <= sp)
    in16 = seen & (db == 0) & (dist <= 16 * WINDOW)
    in4 = seen & (dist <= 4 * WINDOW)
    bias_b[...] = jnp.where(in16 & in4, LN2, jnp.where(in16 | in4, 0.0, NEG))

    for cp in loads(True):
        cp.wait()
    pl.semaphore_wait(barrier, len(peers))

    z_to = [{"z": at_z(1)}, {"z": at_z(-1)}]
    y_to = [{"y": at_y(1)}, {"y": at_y(-1)}]
    partner = {"c": 1 - c}
    last = NZ // 2

    def arrived_all(ref, sem):
        remote(ref, ref, out_sem.at[0], sem, z_to[0]).wait_recv()

    def left_all(ref, sem):
        remote(ref, ref, sem, xd, z_to[0]).wait_send()

    def z_ref(flow, src, way, s):
        if flow < 3:
            lo, n = (2 * flow, 2) if s < last else (2 * flow + way, 1)
            return wz.at[src * NY + y, :, pl.ds(lo * lanes, n * lanes)]
        cols = pl.ds(src * NY, NY) if s < last else pl.ds(src * NY + 2 * way, 2)
        return wog.at[flow - 3, cols]

    def z_copy(flow, way, s, hop):
        ref = z_ref(flow, at_z(-hop if way == 0 else hop), way, s)
        return remote(ref, ref, out_sem.at[flow // 3], zr.at[flow, way, s - 1], z_to[way])

    def z_first(flow):
        for way in (0, 1):
            z_copy(flow, way, 1, 0).start()

    def z_hop(flow, s):
        for way in (0, 1):
            z_copy(flow, way, s, s).wait_recv()
            if s < last:
                z_copy(flow, way, s + 1, s).start()

    def y_copy(kind, slot, col):
        ref = wz.at[at_z(-slot) * NY + at_y(col)]
        split = 3 * lanes
        if kind == 2:
            ref = ref.at[:, pl.ds(0, split)]
        if kind == 3:
            ref = ref.at[:, pl.ds(split, 3 * lanes)]
        to = {"y": at_y(2)} if kind == 4 else y_to[kind % 2]
        return remote(
            ref, ref, out_sem.at[3 if kind < 2 else 2], yr.at[kind, slot] if kind < 2 else yd.at[slot], to
        )

    def y_send(slot):
        y_copy(0, slot, 0).start()
        y_copy(1, slot, 0).start()
        if slot in DIRECT:
            y_copy(4, slot, 0).start()

    def y_relay(slot):
        y_copy(0, slot, -1).wait_recv()
        if slot not in DIRECT:
            y_copy(2, slot, -1).start()
        y_copy(1, slot, 1).wait_recv()
        if slot not in DIRECT:
            y_copy(3, slot, 1).start()

    def y_done(slot):
        y_copy(4, slot, 2).wait_recv()
        row = pl.ds(at_z(-slot) * NY, NY)
        near = min(slot, NZ - slot)
        group = 0 if near <= 4 else 1 if near <= 6 else 2
        remote(wz.at[row, :, other], wz.at[row, :, mine], out_sem.at[4], push_r.at[group], partner).start()

    def o_push(slot):
        row = pl.ds(at_z(-slot) * NY, NY)
        group = X_ORDER.index(slot) // 4
        remote(wog.at[1, row], wog.at[0, row], out_sem.at[5], o_r.at[group], partner).start()

    def arrived(s):
        if s == 0:
            return [0]
        return [s, NZ - s] if s < last else [s]

    def x_copy(kind, slot):
        span = pl.ds(at_z(-slot) * NY, NY)
        way = (0, 1, slot % 2)[kind]
        side = woxs.at[span, :, pl.ds((1 - way) * lanes, lanes)]
        return remote(
            side if kind == 2 else wog.at[0, span], woxm.at[span] if kind == 2 else side, out_sem.at[7],
            xr.at[kind, X_ORDER.index(slot) // 8] if kind < 2 else xd, {"x": at_x(1 if way == 0 else -1)},
        )

    def x_send(slot):
        x_copy(0, slot).start()
        x_copy(1, slot).start()

    def x_relay(group):
        for kind in (0, 1):
            arrived_all(woxm.at[pl.ds(0, 8 * NY)], xr.at[kind, group])
        for slot in X_ORDER[8 * group:8 * group + 8]:
            x_copy(2, slot).start()

    def row_send(item, d):
        ref = wog.at[item, sp]
        return remote(ref, ref, out_sem.at[8], row_r.at[item], {"y": at_y(d)})

    first = z - 4 + lax.rem(z, 2)

    def project(k):
        src = lax.rem(first + 2 * k + NZ, NZ)
        at = pl.multiple_of(src * (NY * shard), 2 * NY * shard)
        w = wz[pl.ds(src * NY, 2 * NY), :, 3 * lanes:].reshape(2 * NY * shard, 3 * lanes)
        return jnp.dot(tok[:, pl.ds(at, 2 * NY * shard)], w, preferred_element_type=F32)

    def first_sends(ref):
        for way in (0, 1):
            remote(ref, ref, out_sem.at[0], zr.at[0, way, 0], {"z": at_z(1 - 2 * way), "c": 1}).start()
        for kind in (0, 1):
            remote(ref, ref, out_sem.at[0], yr.at[kind, 0], {"y": at_y(1 - 2 * kind), "c": 1}).start()

    @pl.when(c == 0)
    def _():
        first_sends(wz.at[sp, :, other])
        for d in (1, 3, 2):
            at = {"y": at_y(d), "c": 1}
            remote(wog.at[1, sp], wog.at[1, sp], out_sem.at[1], row_r.at[1], at).start()
        remote(wog.at[1, sp], wog.at[1, sp], out_sem.at[1], push_r.at[1], partner).start()
        remote(wz.at[sp, :, other], wz.at[sp, :, other], out_sem.at[0], push_r.at[0], partner).start()
        copy_tokens.wait()
        for group in range(4):
            arrived_all(wog.at[0, pl.ds(0, 4 * NY)], o_r.at[group])
            for slot in X_ORDER[4 * group:4 * group + 4]:
                x_send(slot)
            if group == 2:
                arrived_all(wz.at[pl.ds(0, 9 * NY), :, mine], push_r.at[0])
                acc[...] = project(0) + project(1) + project(2) + project(3)
        arrived_all(wz.at[pl.ds(0, 4 * NY), :, mine], push_r.at[1])
        acc[...] += project(-1) + project(4)
        arrived_all(wz.at[pl.ds(0, 3 * NY), :, mine], push_r.at[2])

    @pl.when(c == 1)
    def _():
        first_sends(wz.at[sp, :, mine])
        for d in (1, 3, 2):
            row_send(0, d).start()
        copy_tokens.wait()
        arrived_all(wog.at[1, sp], push_r.at[1])
        arrived_all(wz.at[sp, :, other], push_r.at[0])
        for s in range(1, last + O_LAG + 1):
            if s <= last:
                if s == 1:
                    for way in (0, 1):
                        arrived_all(wz.at[sp], zr.at[0, way, 0])
                        for flow in Z_FLOWS:
                            z_copy(flow, way, 2, 1).start()
                else:
                    for flow in Z_FLOWS:
                        z_hop(flow, s)
                for slot in arrived(s):
                    y_send(slot)
            for item in (0, 1):
                if s == 1:
                    arrived_all(wog.at[0, pl.ds(0, NY - 1)], row_r.at[item])
                    z_first(3 + item)
                elif s > O_LAG:
                    z_hop(3 + item, s - O_LAG)
            for slot in [0] if s == 1 else arrived(s - O_LAG) if s > O_LAG else []:
                x_send(slot)
                o_push(slot)
            if Y_LAG <= s <= last + Y_LAG:
                for slot in arrived(s - Y_LAG):
                    y_relay(slot)
            if Y_DONE <= s <= last + Y_DONE:
                for slot in arrived(s - Y_DONE):
                    y_done(slot)
            if s == 4 + Y_DONE:
                acc[...] = project(0) + project(1) + project(2) + project(3)
            if s == 6 + Y_DONE:
                acc[...] += project(-1) + project(4)
        for s in range(last + O_LAG + 1, last + Y_DONE + 1):
            if s <= last + Y_LAG:
                for slot in arrived(s - Y_LAG):
                    y_relay(slot)
            for slot in arrived(s - Y_DONE):
                y_done(slot)

    x_relay(0)
    qkv = acc[...] + project(5) + project(6)
    for j in range(2):
        side = slice(j * lanes, (j + 1) * lanes)
        kvf[j, WINDOW:, :] = qkv[:, side]
        for e in range(4):
            for b in range(4):
                picked = kvf[j, pl.ds(WINDOW + 4 * b + e, 32, stride=16), :]
                halo[e, 0, 32 * b:32 * b + 32, side] = picked.astype(BF16)

    def prev_copy(e):
        return remote(halo.at[e, 0], halo.at[e, 4], out_sem.at[9], hr.at[0, e], z_to[0])

    def row_copy(e, k, src):
        return remote(halo.at[e, src], halo.at[e, k], out_sem.at[9], hr.at[k, e], {"y": at_y(k)})

    def relay_copy(e, k):
        return remote(halo.at[e, k], halo.at[e, 2], out_sem.at[12], hr.at[2, e], y_to[0 if k == 1 else 1])

    for e in range(4):
        prev_copy(e).start()
        for k in (1, 3):
            @pl.when((y + k < NY) & ((c == 0) | (e < 2)))
            def _():
                row_copy(e, k, 0).start()

    def wrap(e):
        prev_copy(e).wait_recv()
        for k in (1, 3):
            @pl.when(y + k >= NY)
            def _():
                row_copy(e, k, 4).start()

    def pass_on(e):
        row_copy(e, 1, 0).wait_recv()

        @pl.when((y == 2) | ((y < 2) & (e < 2)))
        def _():
            relay_copy(e, 1).start()

        row_copy(e, 3, 0).wait_recv()

        @pl.when((y == 1) | ((y >= 2) & (e >= 2)))
        def _():
            relay_copy(e, 3).start()

    qf[...] = qkv[:, 2 * lanes:].astype(BF16).astype(F32) * (HEAD ** -0.5)
    head0 = lax.broadcasted_iota(jnp.int32, (WINDOW, lanes), 1) < HEAD

    def attend(qb, kb, vb, bias):
        q0 = jnp.where(head0, qb, 0.0).astype(BF16)
        q1 = jnp.where(head0, 0.0, qb).astype(BF16)
        s = nt_dot(jnp.concatenate([q0, q1], 0), kb)
        probs, tops, sums = [], [], []
        for h in range(2):
            sh = s[h * WINDOW:(h + 1) * WINDOW] + bias
            top = jnp.max(sh, axis=1, keepdims=True)
            w = jnp.exp(sh - top)
            tops.append(top)
            sums.append(jnp.sum(w, axis=1, keepdims=True))
            probs.append(w.astype(BF16))
        o = jnp.dot(jnp.concatenate(probs, 0), vb, preferred_element_type=F32)
        out = jnp.where(head0, o[0:WINDOW], o[WINDOW:])
        return out, jnp.where(head0, tops[0], tops[1]), jnp.where(head0, sums[0], sums[1])

    def near_block(i):
        span = slice(i * WINDOW, (i + 1) * WINDOW)
        keys = slice(i * WINDOW, (i + 2) * WINDOW)
        out, top, total = attend(
            qf[span, :], kvf[0, keys, :].astype(BF16), kvf[1, keys, :].astype(BF16), bias_a[min(i, 1)]
        )
        oa[span, :] = out
        ma[span, :] = top
        la[span, :] = total

    for e in range(4):
        wrap(e)
        if e < 2:
            for k in (1, 3):
                @pl.when((y + k < NY) & (c == 1))
                def _():
                    row_copy(e + 2, k, 0).start()
        if e < 3:
            near_block(e + 1)
    x_relay(1)
    for e in range(4):
        pass_on(e)

    for e in range(4):
        for b in range(4):
            for j in range(2):
                tail = halo[e, 1, 32 * b + 24:32 * b + 32, j * lanes:(j + 1) * lanes]
                kvf[j, pl.ds(4 * b + e, 8, stride=16), :] = tail.astype(F32)
    near_block(0)

    for e in range(4):
        row_copy(e, 2, 0).wait_recv()
        pick = [pl.ds(4 * b + e, 32, stride=16) for b in range(4)]
        qb = jnp.concatenate([qf[p, :] for p in pick], 0)
        kvb = halo[e].reshape(5 * WINDOW, 2 * lanes)
        out, top, total = attend(qb, kvb[:, 0:lanes], kvb[:, lanes:], bias_b[...])
        o_a = jnp.concatenate([oa[p, :] for p in pick], 0)
        m_a = jnp.concatenate([ma[p, :] for p in pick], 0)
        l_a = jnp.concatenate([la[p, :] for p in pick], 0)
        peak = jnp.maximum(top, m_a)
        f_b = jnp.exp(top - peak)
        f_a = jnp.exp(m_a - peak)
        denom = f_a * l_a + f_b * total
        res = (f_a * o_a + f_b * out) / denom
        lse = peak + jnp.log(denom)
        for b in range(4):
            att[pick[b], :] = res[32 * b:32 * b + 32]
            lse_rows[pick[b], :] = lse[32 * b:32 * b + 32]

    att_b[...] = att[...].reshape(NX, rows // NX, lanes).astype(BF16)

    def att_copy(d):
        return remote(att_b.at[at_x(d)], att_x.at[NX - d], out_sem.at[10], ar.at[d - 1], {"x": at_x(d)})

    for d in (1, 3, 2):
        att_copy(d).start()
    att_x[0] = att_b[x]
    lse_t = lse_rows[...].T
    lse_v[0:1, :] = lse_t[0:1, :]
    lse_v[1:2, :] = lse_t[HEAD:HEAD + 1, :]
    copy_lse = pltpu.make_async_copy(lse_v, lse_out, load_sem.at[2])
    copy_lse.start()
    groups = 8
    width = NZ * NY // groups
    hrows = rows // NX // 2
    for g in range(groups):
        w_own = wog[0, g * width:(g + 1) * width].reshape(width * shard, lanes)
        part[g] = nt_dot(att_x[0], w_own).reshape(2, hrows, width * shard)
    for d in (1, 3):
        att_copy(NX - d).wait_recv()
    sides = jnp.concatenate([att_x[1], att_x[3]], 1)
    for g in range(groups):
        w_k = woxs[g * width:(g + 1) * width].reshape(width * shard, 2 * lanes)
        part[g] += nt_dot(sides, w_k).reshape(2, hrows, width * shard)
    arrived_all(woxm, xd)
    att_copy(2).wait_recv()

    def core_copy(j):
        at = pl.ds(j * groups // 2, groups // 2)
        return remote(part_b.at[at, 1 - c], theirs.at[at], out_sem.at[11], cr, {"c": 1 - c})

    for g in range(groups):
        span = slice(g * width, (g + 1) * width)
        acc = nt_dot(att_x[2], woxm[span].reshape(width * shard, lanes))
        part_b[g] = (acc.reshape(2, hrows, width * shard) + part[g]).astype(BF16)
        if g % (groups // 2) == groups // 2 - 1:
            core_copy(g * 2 // groups).start()
    pltpu.make_async_copy(part_b.at[:, c], ours, load_sem.at[1]).start()
    remote(part_b.at[:, c], theirs, out_sem.at[11], cr, partner).wait_recv()
    pltpu.make_async_copy(part_b.at[:, c], ours, load_sem.at[1]).wait()
    copy_lse.wait()
    @pl.when(c == 0)
    def _():
        left_all(wz.at[pl.ds(0, 5), :, other], out_sem.at[0])
        left_all(wog.at[0, pl.ds(0, NY)], out_sem.at[1])

    @pl.when(c == 1)
    def _():
        left_all(wz.at[pl.ds(0, NZ - 1)], out_sem.at[0])
        left_all(wog.at[:, pl.ds(0, (NZ - 1) * NY)], out_sem.at[1])
        left_all(wz.at[pl.ds(0, 2 * NZ - 2)], out_sem.at[3])
        left_all(wz.at[pl.ds(0, NZ)], out_sem.at[2])
        left_all(wz.at[:, :, mine], out_sem.at[4])
        left_all(wog.at[0], out_sem.at[5])
        left_all(wog.at[0, pl.ds(0, NY - 1)], out_sem.at[8])

    left_all(wz.at[:, :, mine], out_sem.at[7])
    left_all(halo.at[:, pl.ds(0, 3)], out_sem.at[9])
    left_all(halo.at[0, pl.ds(0, 2)], out_sem.at[12])

    @pl.when((y == 1) | (y == 2))
    def _():
        left_all(halo.at[:, 0], out_sem.at[12])

    left_all(att_x.at[pl.ds(1, NX - 1)], out_sem.at[10])
    left_all(part_b.at[:, c], out_sem.at[11])


def sum_kernel(ours, theirs, lse, mixed, lse_out):
    wide = ours.shape[2]
    for g in range(ours.shape[0]):
        total = ours[g].astype(F32) + theirs[g].astype(F32)
        mixed[:, g * wide:(g + 1) * wide] = total.astype(BF16)
    lse_out[...] = lse[...]


def shards(tokens, w_query, w_key, w_value, w_out):
    rows, depth = tokens.shape
    shard, lanes = w_query.shape
    n_sp = NZ * NY
    groups = 8
    wide = n_sp // groups * shard
    vmem = pl.BlockSpec(memory_space=pltpu.VMEM)
    anywhere = pl.BlockSpec(memory_space=pl.ANY)
    dma = pltpu.SemaphoreType.DMA
    ours, theirs, lse = pl.pallas_call(
        layer_kernel,
        name="layer",
        out_shape=(
            jax.ShapeDtypeStruct((groups, rows // 8, wide), BF16),
            jax.ShapeDtypeStruct((groups, rows // 8, wide), BF16),
            jax.ShapeDtypeStruct((2, rows), F32),
        ),
        in_specs=[pl.BlockSpec(memory_space=pl.ANY)] * 5,
        out_specs=(anywhere, anywhere, anywhere),
        scratch_shapes=[
            pltpu.VMEM((rows, depth), BF16),
            pltpu.VMEM((rows, 3 * lanes), F32),
            pltpu.VMEM((n_sp, shard, 6 * lanes), BF16),
            pltpu.VMEM((2, n_sp, shard, lanes), BF16),
            pltpu.VMEM((n_sp, shard, 2 * lanes), BF16),
            pltpu.VMEM((n_sp, shard, lanes), BF16),
            pltpu.VMEM((4, 5, WINDOW, 2 * lanes), BF16),
            pltpu.VMEM((rows, lanes), F32),
            pltpu.VMEM((2, WINDOW + rows, lanes), F32),
            pltpu.VMEM((rows, lanes), F32),
            pltpu.VMEM((rows, lanes), F32),
            pltpu.VMEM((rows, lanes), F32),
            pltpu.VMEM((rows, lanes), F32),
            pltpu.VMEM((rows, lanes), F32),
            pltpu.VMEM((2, rows), F32),
            pltpu.VMEM((NX, rows // NX, lanes), BF16),
            pltpu.VMEM((NX, rows // NX, lanes), BF16),
            pltpu.VMEM((groups, 2, rows // NX // 2, wide), F32),
            pltpu.VMEM((groups, 2, rows // NX // 2, wide), BF16),
            pltpu.VMEM((2, WINDOW, 2 * WINDOW), F32),
            pltpu.VMEM((WINDOW, 5 * WINDOW), F32),
            dma((5,)),
            dma((13,)),
            dma((2,)),
            dma((5, 2, NZ // 2)),
            dma((2, NZ)),
            dma((NZ,)),
            dma((3,)),
            dma((4,)),
            dma((2, 2)),
            dma,
            dma((4, 4)),
            dma((3,)),
            dma,
        ],
        compiler_params=pltpu.CompilerParams(
            collective_id=0, has_side_effects=True, vmem_limit_bytes=60 * 1024 * 1024
        ),
    )(tokens, w_query, w_key, w_value, w_out.T)
    return pl.pallas_call(
        sum_kernel,
        name="total",
        out_shape=(
            jax.ShapeDtypeStruct((rows // 8, depth), BF16),
            jax.ShapeDtypeStruct((2, rows), F32),
        ),
        in_specs=[vmem] * 3,
        out_specs=(vmem, vmem),
    )(ours, theirs, lse)


def solution(mesh):
    torus = Mesh(mesh.devices.reshape(NZ, NY, NX, 2), ("z", "y", "x", "c"))
    in_specs = (P(SP, None), P(SP, TP), P(SP, TP), P(SP, TP), P(TP, SP))
    out_specs = (P(SP + TP, None), P(TP, SP))
    return jax.shard_map(
        shards, mesh=torus, in_specs=in_specs, out_specs=out_specs, check_vma=False
    )
```

```python
import jax
import jax.numpy as jnp
from jax import lax
from jax.experimental import pallas as pl
from jax.experimental.pallas import tpu as pltpu
from jax.sharding import Mesh
from jax.sharding import PartitionSpec as P

HEAD = 64
WINDOW = 128
NZ = 16
NY = 4
NX = 4
MESH = pl.DeviceIdType.MESH
SP = ("z", "y")
TP = ("x", "c")
NEG = -1e30
LN2 = 0.6931471805599453
F32 = jnp.float32
BF16 = jnp.bfloat16
X_ORDER = [0] + [v for s in range(1, NZ // 2) for v in (s, NZ - s)] + [NZ // 2]


O_LAG = 1
Y_LAG = 1
Y_DONE = 3
Z_FLOWS = (2, 1, 0)
DIRECT = (NZ // 2,)


def nt_dot(a, b):
    return lax.dot_general(a, b, (((1,), (1,)), ((), ())), preferred_element_type=F32)


def remote(src, dst, send, recv, device):
    return pltpu.make_async_remote_copy(
        src_ref=src, dst_ref=dst, send_sem=send, recv_sem=recv, device_id=device, device_id_type=MESH
    )


def layer_kernel(
    tokens, wq, wk_in, wv, wo, ours, theirs, lse_out,
    tok, acc, wz, wog, woxs, woxm, halo, qf, kvf, oa, ma, la, att, lse_rows, lse_v, att_b, att_x, part, part_b,
    bias_a, bias_b,
    load_sem, out_sem, row_r, zr, yr, yd, push_r, o_r, xr, xd, hr, ar, cr,
):
    z, y, x, c = (lax.axis_index(n) for n in ("z", "y", "x", "c"))
    sp = z * NY + y
    shard, lanes = wk_in.shape
    rows = tokens.shape[0]
    other = pl.ds(0, 3 * lanes)
    mine = pl.ds(3 * lanes, 3 * lanes)

    def load(src, dst, k):
        return pltpu.make_async_copy(src, dst, load_sem.at[k])

    def loads(first):
        lo, slot = (0, 1) if first else (3 * lanes, 0)
        return [
            load(wk_in, wz.at[sp, :, pl.ds(lo, lanes)], 1),
            load(wv, wz.at[sp, :, pl.ds(lo + lanes, lanes)], 2),
            load(wq, wz.at[sp, :, pl.ds(lo + 2 * lanes, lanes)], 3),
            load(wo, wog.at[slot, sp], 4),
        ]

    for core in (0, 1):
        @pl.when(c == core)
        def _():
            for cp in loads(core == 0):
                cp.start()
    copy_tokens = load(tokens, tok, 0)
    copy_tokens.start()

    def at_z(d):
        return lax.rem(z + d + NZ, NZ)

    def at_y(d):
        return lax.rem(y + d + NY, NY)

    def at_x(d):
        return lax.rem(x + d + NX, NX)

    barrier = pltpu.get_barrier_semaphore()
    peers = [{"z": at_z(1)}, {"z": at_z(-1)}]
    peers += [{"y": at_y(d)} for d in range(1, NY)]
    peers += [{"x": at_x(d)} for d in range(1, NX)]
    peers += [{"c": 1 - c}]
    peers += [{"z": at_z(d), "c": 1 - c} for d in (1, -1)] + [{"y": at_y(d), "c": 1 - c} for d in range(1, NY)]
    for peer in peers:
        pl.semaphore_signal(barrier, inc=1, device_id=peer, device_id_type=MESH)
    r = lax.broadcasted_iota(jnp.int32, (WINDOW, 2 * WINDOW), 0)
    k_ = lax.broadcasted_iota(jnp.int32, (WINDOW, 2 * WINDOW), 1)
    dist = WINDOW + r - k_
    near = (dist >= 0) & (dist <= WINDOW)
    bias_a[1] = jnp.where(near, 0.0, NEG)
    bias_a[0] = jnp.where(near & ((k_ >= WINDOW) | (sp > 0)), 0.0, NEG)
    r = lax.broadcasted_iota(jnp.int32, (WINDOW, 5 * WINDOW), 0)
    k_ = lax.broadcasted_iota(jnp.int32, (WINDOW, 5 * WINDOW), 1)
    back = lax.shift_right_logical(k_, 7)
    kr = k_ & 127
    db = lax.shift_right_logical(r, 5) - lax.shift_right_logical(kr, 5)
    dist = rows * back + 16 * ((r & 31) - (kr & 31)) + 4 * db
    seen = (dist >= 0) & (back <= sp)
    in16 = seen & (db == 0) & (dist <= 16 * WINDOW)
    in4 = seen & (dist <= 4 * WINDOW)
    bias_b[...] = jnp.where(in16 & in4, LN2, jnp.where(in16 | in4, 0.0, NEG))

    for cp in loads(True):
        cp.wait()
    pl.semaphore_wait(barrier, len(peers))

    z_to = [{"z": at_z(1)}, {"z": at_z(-1)}]
    y_to = [{"y": at_y(1)}, {"y": at_y(-1)}]
    partner = {"c": 1 - c}
    last = NZ // 2

    def arrived_all(ref, sem):
        remote(ref, ref, out_sem.at[0], sem, z_to[0]).wait_recv()

    def left_all(ref, sem):
        remote(ref, ref, sem, xd, z_to[0]).wait_send()

    def z_ref(flow, src, way, s):
        if flow < 3:
            lo, n = (2 * flow, 2) if s < last else (2 * flow + way, 1)
            return wz.at[src * NY + y, :, pl.ds(lo * lanes, n * lanes)]
        cols = pl.ds(src * NY, NY) if s < last else pl.ds(src * NY + 2 * way, 2)
        return wog.at[flow - 3, cols]

    def z_copy(flow, way, s, hop):
        ref = z_ref(flow, at_z(-hop if way == 0 else hop), way, s)
        return remote(ref, ref, out_sem.at[flow // 3], zr.at[flow, way, s - 1], z_to[way])

    def z_first(flow):
        for way in (0, 1):
            z_copy(flow, way, 1, 0).start()

    def z_hop(flow, s):
        for way in (0, 1):
            z_copy(flow, way, s, s).wait_recv()
            if s < last:
                z_copy(flow, way, s + 1, s).start()

    def y_copy(kind, slot, col):
        ref = wz.at[at_z(-slot) * NY + at_y(col)]
        split = 3 * lanes
        if kind == 2:
            ref = ref.at[:, pl.ds(0, split)]
        if kind == 3:
            ref = ref.at[:, pl.ds(split, 3 * lanes)]
        to = {"y": at_y(2)} if kind == 4 else y_to[kind % 2]
        return remote(
            ref, ref, out_sem.at[3 if kind < 2 else 2],
            yr.at[kind, min(slot, NZ - slot)] if kind < 2 else yd.at[min(slot, NZ - slot)], to,
        )

    def y_send(slot):
        y_copy(0, slot, 0).start()
        y_copy(1, slot, 0).start()
        if slot in DIRECT:
            y_copy(4, slot, 0).start()

    def y_relay(step):
        for kind, col in ((0, -1), (1, 1)):
            arrived_all(wz.at[pl.ds(0, len(arrived(step)))], yr.at[kind, step])
            for slot in arrived(step):
                if slot not in DIRECT:
                    y_copy(kind + 2, slot, col).start()

    def y_done(step):
        arrived_all(wz.at[pl.ds(0, len(arrived(step)))], yd.at[step])
        for slot in arrived(step):
            y_push(slot)

    def y_push(slot):
        row = pl.ds(at_z(-slot) * NY, NY)
        near = min(slot, NZ - slot)
        group = 0 if near <= 4 else 1 if near <= 6 else 2
        remote(wz.at[row, :, other], wz.at[row, :, mine], out_sem.at[4], push_r.at[group], partner).start()

    def o_push(slot):
        row = pl.ds(at_z(-slot) * NY, NY)
        group = X_ORDER.index(slot) // 4
        remote(wog.at[1, row], wog.at[0, row], out_sem.at[5], o_r.at[group], partner).start()

    def arrived(s):
        if s == 0:
            return [0]
        return [s, NZ - s] if s < last else [s]

    def x_copy(kind, slot):
        span = pl.ds(at_z(-slot) * NY, NY)
        way = (0, 1, slot % 2)[kind]
        side = woxs.at[span, :, pl.ds((1 - way) * lanes, lanes)]
        return remote(
            side if kind == 2 else wog.at[0, span], woxm.at[span] if kind == 2 else side, out_sem.at[7],
            xr.at[kind, X_ORDER.index(slot) // 8] if kind < 2 else xd, {"x": at_x(1 if way == 0 else -1)},
        )

    def x_send(slot):
        x_copy(0, slot).start()
        x_copy(1, slot).start()

    def x_relay(group):
        for kind in (0, 1):
            arrived_all(woxm.at[pl.ds(0, 8 * NY)], xr.at[kind, group])
        for slot in X_ORDER[8 * group:8 * group + 8]:
            x_copy(2, slot).start()

    def row_send(item, d):
        ref = wog.at[item, sp]
        return remote(ref, ref, out_sem.at[8], row_r.at[item], {"y": at_y(d)})

    first = z - 4 + lax.rem(z, 2)

    def project(k):
        src = lax.rem(first + 2 * k + NZ, NZ)
        at = pl.multiple_of(src * (NY * shard), 2 * NY * shard)
        w = wz[pl.ds(src * NY, 2 * NY), :, 3 * lanes:].reshape(2 * NY * shard, 3 * lanes)
        return jnp.dot(tok[:, pl.ds(at, 2 * NY * shard)], w, preferred_element_type=F32)

    def first_sends(ref):
        for way in (0, 1):
            remote(ref, ref, out_sem.at[0], zr.at[0, way, 0], {"z": at_z(1 - 2 * way), "c": 1}).start()
        for kind in (0, 1):
            remote(ref, ref, out_sem.at[0], yr.at[kind, 0], {"y": at_y(1 - 2 * kind), "c": 1}).start()

    @pl.when(c == 0)
    def _():
        first_sends(wz.at[sp, :, other])
        for d in (1, 3, 2):
            at = {"y": at_y(d), "c": 1}
            remote(wog.at[1, sp], wog.at[1, sp], out_sem.at[1], row_r.at[1], at).start()
        remote(wog.at[1, sp], wog.at[1, sp], out_sem.at[1], push_r.at[1], partner).start()
        remote(wz.at[sp, :, other], wz.at[sp, :, other], out_sem.at[0], push_r.at[0], partner).start()
        copy_tokens.wait()
        for group in range(4):
            arrived_all(wog.at[0, pl.ds(0, 4 * NY)], o_r.at[group])
            for slot in X_ORDER[4 * group:4 * group + 4]:
                x_send(slot)
            if group == 2:
                arrived_all(wz.at[pl.ds(0, 9 * NY), :, mine], push_r.at[0])
                acc[...] = project(0) + project(1) + project(2) + project(3)
        arrived_all(wz.at[pl.ds(0, 4 * NY), :, mine], push_r.at[1])
        acc[...] += project(-1) + project(4)
        arrived_all(wz.at[pl.ds(0, 3 * NY), :, mine], push_r.at[2])

    @pl.when(c == 1)
    def _():
        first_sends(wz.at[sp, :, mine])
        for d in (1, 3, 2):
            row_send(0, d).start()
        copy_tokens.wait()
        arrived_all(wog.at[1, sp], push_r.at[1])
        arrived_all(wz.at[sp, :, other], push_r.at[0])
        for s in range(1, last + O_LAG + 1):
            if s <= last:
                if s == 1:
                    for way in (0, 1):
                        arrived_all(wz.at[sp], zr.at[0, way, 0])
                        for flow in Z_FLOWS:
                            z_copy(flow, way, 2, 1).start()
                else:
                    for flow in Z_FLOWS:
                        z_hop(flow, s)
                for slot in arrived(s):
                    y_send(slot)
            for item in (0, 1):
                if s == 1:
                    arrived_all(wog.at[0, pl.ds(0, NY - 1)], row_r.at[item])
                    z_first(3 + item)
                elif s > O_LAG:
                    z_hop(3 + item, s - O_LAG)
            for slot in [0] if s == 1 else arrived(s - O_LAG) if s > O_LAG else []:
                x_send(slot)
                o_push(slot)
            if Y_LAG <= s <= last + Y_LAG:
                y_relay(s - Y_LAG)
            if Y_DONE <= s <= last + Y_DONE:
                y_done(s - Y_DONE)
            if s == 4 + Y_DONE:
                acc[...] = project(0) + project(1) + project(2) + project(3)
            if s == 6 + Y_DONE:
                acc[...] += project(-1) + project(4)
        for s in range(last + O_LAG + 1, last + Y_DONE + 1):
            if s <= last + Y_LAG:
                y_relay(s - Y_LAG)
            y_done(s - Y_DONE)

    x_relay(0)
    qkv = acc[...] + project(5) + project(6)
    for j in range(2):
        side = slice(j * lanes, (j + 1) * lanes)
        kvf[j, WINDOW:, :] = qkv[:, side]
        for e in range(4):
            for b in range(4):
                picked = kvf[j, pl.ds(WINDOW + 4 * b + e, 32, stride=16), :]
                halo[e, 0, 32 * b:32 * b + 32, side] = picked.astype(BF16)

    def prev_copy(e):
        return remote(halo.at[e, 0], halo.at[e, 4], out_sem.at[9], hr.at[0, e], z_to[0])

    def row_copy(e, k, src):
        return remote(halo.at[e, src], halo.at[e, k], out_sem.at[9], hr.at[k, e], {"y": at_y(k)})

    def relay_copy(e, k):
        return remote(halo.at[e, k], halo.at[e, 2], out_sem.at[12], hr.at[2, e], y_to[0 if k == 1 else 1])

    for e in range(4):
        prev_copy(e).start()
        for k in (1, 3):
            @pl.when((y + k < NY) & ((c == 0) | (e < 2)))
            def _():
                row_copy(e, k, 0).start()

    def wrap(e):
        prev_copy(e).wait_recv()
        for k in (1, 3):
            @pl.when(y + k >= NY)
            def _():
                row_copy(e, k, 4).start()

    def pass_on(e):
        row_copy(e, 1, 0).wait_recv()

        @pl.when((y == 2) | ((y < 2) & (e < 2)))
        def _():
            relay_copy(e, 1).start()

        row_copy(e, 3, 0).wait_recv()

        @pl.when((y == 1) | ((y >= 2) & (e >= 2)))
        def _():
            relay_copy(e, 3).start()

    qf[...] = qkv[:, 2 * lanes:].astype(BF16).astype(F32) * (HEAD ** -0.5)
    head0 = lax.broadcasted_iota(jnp.int32, (WINDOW, lanes), 1) < HEAD

    def attend(qb, kb, vb, bias):
        q0 = jnp.where(head0, qb, 0.0).astype(BF16)
        q1 = jnp.where(head0, 0.0, qb).astype(BF16)
        s = nt_dot(jnp.concatenate([q0, q1], 0), kb)
        probs, tops, sums = [], [], []
        for h in range(2):
            sh = s[h * WINDOW:(h + 1) * WINDOW] + bias
            top = jnp.max(sh, axis=1, keepdims=True)
            w = jnp.exp(sh - top)
            tops.append(top)
            sums.append(jnp.sum(w, axis=1, keepdims=True))
            probs.append(w.astype(BF16))
        o = jnp.dot(jnp.concatenate(probs, 0), vb, preferred_element_type=F32)
        out = jnp.where(head0, o[0:WINDOW], o[WINDOW:])
        return out, jnp.where(head0, tops[0], tops[1]), jnp.where(head0, sums[0], sums[1])

    def near_block(i):
        span = slice(i * WINDOW, (i + 1) * WINDOW)
        keys = slice(i * WINDOW, (i + 2) * WINDOW)
        out, top, total = attend(
            qf[span, :], kvf[0, keys, :].astype(BF16), kvf[1, keys, :].astype(BF16), bias_a[min(i, 1)]
        )
        oa[span, :] = out
        ma[span, :] = top
        la[span, :] = total

    for e in range(4):
        wrap(e)
        if e < 2:
            for k in (1, 3):
                @pl.when((y + k < NY) & (c == 1))
                def _():
                    row_copy(e + 2, k, 0).start()
        if e < 3:
            near_block(e + 1)
    x_relay(1)
    for e in range(4):
        pass_on(e)

    for e in range(4):
        for b in range(4):
            for j in range(2):
                tail = halo[e, 1, 32 * b + 24:32 * b + 32, j * lanes:(j + 1) * lanes]
                kvf[j, pl.ds(4 * b + e, 8, stride=16), :] = tail.astype(F32)
    near_block(0)

    for e in range(4):
        row_copy(e, 2, 0).wait_recv()
        pick = [pl.ds(4 * b + e, 32, stride=16) for b in range(4)]
        qb = jnp.concatenate([qf[p, :] for p in pick], 0)
        kvb = halo[e].reshape(5 * WINDOW, 2 * lanes)
        out, top, total = attend(qb, kvb[:, 0:lanes], kvb[:, lanes:], bias_b[...])
        o_a = jnp.concatenate([oa[p, :] for p in pick], 0)
        m_a = jnp.concatenate([ma[p, :] for p in pick], 0)
        l_a = jnp.concatenate([la[p, :] for p in pick], 0)
        peak = jnp.maximum(top, m_a)
        f_b = jnp.exp(top - peak)
        f_a = jnp.exp(m_a - peak)
        denom = f_a * l_a + f_b * total
        res = (f_a * o_a + f_b * out) / denom
        lse = peak + jnp.log(denom)
        for b in range(4):
            att[pick[b], :] = res[32 * b:32 * b + 32]
            lse_rows[pick[b], :] = lse[32 * b:32 * b + 32]

    att_b[...] = att[...].reshape(NX, rows // NX, lanes).astype(BF16)

    def att_copy(d):
        return remote(att_b.at[at_x(d)], att_x.at[NX - d], out_sem.at[10], ar.at[d - 1], {"x": at_x(d)})

    for d in (1, 3, 2):
        att_copy(d).start()
    att_x[0] = att_b[x]
    lse_t = lse_rows[...].T
    lse_v[0:1, :] = lse_t[0:1, :]
    lse_v[1:2, :] = lse_t[HEAD:HEAD + 1, :]
    copy_lse = pltpu.make_async_copy(lse_v, lse_out, load_sem.at[2])
    copy_lse.start()
    groups = 8
    width = NZ * NY // groups
    hrows = rows // NX // 2
    for g in range(groups):
        w_own = wog[0, g * width:(g + 1) * width].reshape(width * shard, lanes)
        part[g] = nt_dot(att_x[0], w_own).reshape(2, hrows, width * shard)
    for d in (1, 3):
        att_copy(NX - d).wait_recv()
    sides = jnp.concatenate([att_x[1], att_x[3]], 1)
    for g in range(groups):
        w_k = woxs[g * width:(g + 1) * width].reshape(width * shard, 2 * lanes)
        part[g] += nt_dot(sides, w_k).reshape(2, hrows, width * shard)
    arrived_all(woxm, xd)
    att_copy(2).wait_recv()

    def core_copy(j):
        at = pl.ds(j * groups // 2, groups // 2)
        return remote(part_b.at[at, 1 - c], theirs.at[at], out_sem.at[11], cr, {"c": 1 - c})

    for g in range(groups):
        span = slice(g * width, (g + 1) * width)
        acc = nt_dot(att_x[2], woxm[span].reshape(width * shard, lanes))
        part_b[g] = (acc.reshape(2, hrows, width * shard) + part[g]).astype(BF16)
        if g % (groups // 2) == groups // 2 - 1:
            core_copy(g * 2 // groups).start()
    pltpu.make_async_copy(part_b.at[:, c], ours, load_sem.at[1]).start()
    remote(part_b.at[:, c], theirs, out_sem.at[11], cr, partner).wait_recv()
    pltpu.make_async_copy(part_b.at[:, c], ours, load_sem.at[1]).wait()
    copy_lse.wait()
    @pl.when(c == 0)
    def _():
        left_all(wz.at[pl.ds(0, 5), :, other], out_sem.at[0])
        left_all(wog.at[0, pl.ds(0, NY)], out_sem.at[1])

    @pl.when(c == 1)
    def _():
        left_all(wz.at[pl.ds(0, NZ - 1)], out_sem.at[0])
        left_all(wog.at[:, pl.ds(0, (NZ - 1) * NY)], out_sem.at[1])
        left_all(wz.at[pl.ds(0, 2 * NZ - 2)], out_sem.at[3])
        left_all(wz.at[pl.ds(0, NZ)], out_sem.at[2])
        left_all(wz.at[:, :, mine], out_sem.at[4])
        left_all(wog.at[0], out_sem.at[5])
        left_all(wog.at[0, pl.ds(0, NY - 1)], out_sem.at[8])

    left_all(wz.at[:, :, mine], out_sem.at[7])
    left_all(halo.at[:, pl.ds(0, 3)], out_sem.at[9])
    left_all(halo.at[0, pl.ds(0, 2)], out_sem.at[12])

    @pl.when((y == 1) | (y == 2))
    def _():
        left_all(halo.at[:, 0], out_sem.at[12])

    left_all(att_x.at[pl.ds(1, NX - 1)], out_sem.at[10])
    left_all(part_b.at[:, c], out_sem.at[11])


def sum_kernel(ours, theirs, lse, mixed, lse_out):
    wide = ours.shape[2]
    for g in range(ours.shape[0]):
        total = ours[g].astype(F32) + theirs[g].astype(F32)
        mixed[:, g * wide:(g + 1) * wide] = total.astype(BF16)
    lse_out[...] = lse[...]


def shards(tokens, w_query, w_key, w_value, w_out):
    rows, depth = tokens.shape
    shard, lanes = w_query.shape
    n_sp = NZ * NY
    groups = 8
    wide = n_sp // groups * shard
    vmem = pl.BlockSpec(memory_space=pltpu.VMEM)
    anywhere = pl.BlockSpec(memory_space=pl.ANY)
    dma = pltpu.SemaphoreType.DMA
    ours, theirs, lse = pl.pallas_call(
        layer_kernel,
        name="layer",
        out_shape=(
            jax.ShapeDtypeStruct((groups, rows // 8, wide), BF16),
            jax.ShapeDtypeStruct((groups, rows // 8, wide), BF16),
            jax.ShapeDtypeStruct((2, rows), F32),
        ),
        in_specs=[pl.BlockSpec(memory_space=pl.ANY)] * 5,
        out_specs=(anywhere, anywhere, anywhere),
        scratch_shapes=[
            pltpu.VMEM((rows, depth), BF16),
            pltpu.VMEM((rows, 3 * lanes), F32),
            pltpu.VMEM((n_sp, shard, 6 * lanes), BF16),
            pltpu.VMEM((2, n_sp, shard, lanes), BF16),
            pltpu.VMEM((n_sp, shard, 2 * lanes), BF16),
            pltpu.VMEM((n_sp, shard, lanes), BF16),
            pltpu.VMEM((4, 5, WINDOW, 2 * lanes), BF16),
            pltpu.VMEM((rows, lanes), F32),
            pltpu.VMEM((2, WINDOW + rows, lanes), F32),
            pltpu.VMEM((rows, lanes), F32),
            pltpu.VMEM((rows, lanes), F32),
            pltpu.VMEM((rows, lanes), F32),
            pltpu.VMEM((rows, lanes), F32),
            pltpu.VMEM((rows, lanes), F32),
            pltpu.VMEM((2, rows), F32),
            pltpu.VMEM((NX, rows // NX, lanes), BF16),
            pltpu.VMEM((NX, rows // NX, lanes), BF16),
            pltpu.VMEM((groups, 2, rows // NX // 2, wide), F32),
            pltpu.VMEM((groups, 2, rows // NX // 2, wide), BF16),
            pltpu.VMEM((2, WINDOW, 2 * WINDOW), F32),
            pltpu.VMEM((WINDOW, 5 * WINDOW), F32),
            dma((5,)),
            dma((13,)),
            dma((2,)),
            dma((5, 2, NZ // 2)),
            dma((2, NZ // 2 + 1)),
            dma((NZ // 2 + 1,)),
            dma((3,)),
            dma((4,)),
            dma((2, 2)),
            dma,
            dma((4, 4)),
            dma((3,)),
            dma,
        ],
        compiler_params=pltpu.CompilerParams(
            collective_id=0, has_side_effects=True, vmem_limit_bytes=60 * 1024 * 1024
        ),
    )(tokens, w_query, w_key, w_value, w_out.T)
    return pl.pallas_call(
        sum_kernel,
        name="total",
        out_shape=(
            jax.ShapeDtypeStruct((rows // 8, depth), BF16),
            jax.ShapeDtypeStruct((2, rows), F32),
        ),
        in_specs=[vmem] * 3,
        out_specs=(vmem, vmem),
    )(ours, theirs, lse)


def solution(mesh):
    torus = Mesh(mesh.devices.reshape(NZ, NY, NX, 2), ("z", "y", "x", "c"))
    in_specs = (P(SP, None), P(SP, TP), P(SP, TP), P(SP, TP), P(TP, SP))
    out_specs = (P(SP + TP, None), P(TP, SP))
    return jax.shard_map(
        shards, mesh=torus, in_specs=in_specs, out_specs=out_specs, check_vma=False
    )
```
